256 devices in a mesh: sp: 64 (over z, x, core), tp: 4 (over y).
Axes of the slice: x: 4, y: 4, z: 8, core: 2. Of those that a mesh axis runs over, the one named last changes fastest.
Arguments:
- stream: bfloat16 [32768, 2048], P(('sp', 'tp')), may hold values from -6 to 6
- queries: bfloat16 [32768, 512], P('sp', 'tp'), may hold values from -6 to 6
- key_rows: bfloat16 [32768, 512], P('sp', 'tp'), may hold values from -6 to 6
- values: bfloat16 [32768, 1024], P('sp', 'tp'), may hold values from -6 to 6
- out_gate: bfloat16 [32768, 1024], P('sp', 'tp'), may hold values from -6 to 6
- fwd_decay: float32 [32768, 512], P('sp', 'tp'), may hold values from -14 to 14
- bwd_decay: float32 [32768, 512], P('sp', 'tp'), may hold values from -14 to 14
- head_gain: float32 [1024], P('tp'), may hold values from 0.1 to 1.9
- out_proj: bfloat16 [1024, 2048], replicated, may hold values from -0.1875 to 0.1875
- mix_gain: float32 [2048], replicated, may hold values from 0.1 to 1.9
- ffn_gain: float32 [2048], replicated, may hold values from 0.1 to 1.9
- moe_gain: float32 [2048], replicated, may hold values from 0.1 to 1.9
- routes: int32 [32768, 2], P(('sp', 'tp')), may hold values from 0 to 63, all different within a row; in each aligned block of 128 rows (0 to 127, 128 to 255, ...) at most 6 rows name the same one
- route_weight: float32 [32768, 2], P(('sp', 'tp')), may hold values from 0.25 to 2.5
- expert_gate: bfloat16 [64, 2048, 1024], P('sp', None, 'tp'), may hold values from -0.125 to 0.125
- expert_up: bfloat16 [64, 2048, 1024], P('sp', None, 'tp'), may hold values from -0.125 to 0.125
- expert_down: bfloat16 [64, 1024, 2048], P('sp', 'tp'), may hold values from -0.1875 to 0.1875
- shared_gate: bfloat16 [2048, 512], P(None, 'tp'), may hold values from -0.125 to 0.125
- shared_up: bfloat16 [2048, 512], P(None, 'tp'), may hold values from -0.125 to 0.125
- shared_down: bfloat16 [512, 2048], P('tp'), may hold values from -0.25 to 0.25
Outputs:
- updated: bfloat16 [32768, 2048], P(('sp', 'tp'))
The draws below stay inside these ranges and needn't reach their ends.
Inputs may be any that keep to these rules, and one draw needn't show every extreme that they name: `routes`: each row names 2 different experts. Among the rows of one device no expert is named more than 6 times, and in every draw some device names some expert exactly 6 times.
All inputs are finite; a program needn't handle non-finite values.
Results may differ from the reference program's by a relative error of at most 0.023.
Values may be sent and summed in bfloat16 or wider, within the bound.
No kernel may reach another device: no remote copies, remote signals or barrier semaphores. Data moves between devices by JAX's collectives and lax.ppermute only.
A program may use at most 128 MiB of HBM per device.

```python
import math
import jax
import jax.numpy as jnp
import numpy as np
from jax import lax

D = 2048
HEAD_TOTAL = 8
KEY_CHANNELS = 64
DV = 128
BLK = 64
FE = 1024
SH = 512
TOPK = 2
TOK_DEV = 128
TOKEN_COUNT = 32768
HV = 1024
EXPERTS = 64
CAP = 6
PARTS_SIZE = 4


def decay_law(key):
    head_key, chan_key, dev_key, jitter_key, position_key, fraction_key = jax.random.split(key, 6)
    slow_share = 0.5
    slow_heads = jax.random.uniform(head_key, (HEAD_TOTAL,)) < slow_share
    head_rate = jnp.where(slow_heads, 0.6 / TOKEN_COUNT, 2.5 / BLK)
    channel_rate = jnp.repeat(head_rate, KEY_CHANNELS) * jnp.exp(jax.random.uniform(chan_key, (HEAD_TOTAL * KEY_CHANNELS,), minval=-0.5, maxval=0.5))
    device_factor = jnp.exp(jax.random.uniform(dev_key, (TOKEN_COUNT // TOK_DEV, 1), minval=-0.7, maxval=0.7))
    rates = jnp.repeat(device_factor, TOK_DEV, axis=0) * channel_rate[None, :]
    preactivation = -jnp.log(jnp.expm1(16.0 * rates))
    preactivation = preactivation + jax.random.uniform(jitter_key, (TOKEN_COUNT, HEAD_TOTAL * KEY_CHANNELS), minval=-1.0, maxval=1.0)
    spike_rows = jax.random.randint(position_key, (2,), 0, TOKEN_COUNT)
    spike_fraction = jax.random.uniform(fraction_key, (2, HEAD_TOTAL * KEY_CHANNELS), minval=0.2, maxval=0.5)
    spike_preactivation = -jnp.log(jnp.expm1(-16.0 * jnp.log(1.0 - spike_fraction)))
    preactivation = preactivation.at[spike_rows].set(spike_preactivation)
    return jnp.clip(preactivation, -14.0, 14.0).astype(jnp.float32)


def draw_fwd_decay(key, part):
    return decay_law(jax.random.fold_in(key, 11))


def draw_bwd_decay(key, part):
    return decay_law(jax.random.fold_in(key, 23))


def levels(own_key, dims, cuts, low, high):
    gain = 1.0
    for dim, blocks in cuts:
        draws = jax.random.uniform(jax.random.fold_in(jax.random.fold_in(own_key, 6), dim), (blocks,), jnp.float32, low / len(cuts), high / len(cuts))
        gain = gain * jnp.repeat(jnp.exp(draws), dims[dim] // blocks).reshape((-1,) + (1,) * (len(dims) - 1 - dim))
    return gain


def deal_out(key, own, number, rows, amount, top, most, lean):
    sequence = jax.random.permutation(key, amount)
    heavy_load, ordinary = portions_of(amount, rows * top, most, lean, True), portions_of(amount, rows * top, most, lean, False)
    places = jnp.arange(amount)

    def named(tallies, rotation):
        used = int((tallies > 0).sum())
        fixed = max(1, used // 4)
        shifted = fixed + (places - fixed + rotation * (used - fixed)) % max(1, amount - fixed)
        return jnp.zeros((amount,), jnp.int32).at[sequence[jnp.where(places < fixed, places, shifted)]].set(jnp.asarray(tallies, jnp.int32))

    tallies = jnp.where(number % 4 == 0, named(heavy_load, number // 4), named(ordinary, number - number // 4 - 1))
    mixed = jax.random.permutation(jax.random.fold_in(own, 3), amount)
    giver, taker = mixed[0:amount // 2 * 2:2], mixed[1:amount // 2 * 2:2]
    room = jnp.minimum(tallies[giver] - 1, most - tallies[taker]) // 2
    room = jnp.where((giver == sequence[0]) | (taker == sequence[0]) | (tallies[taker] == 0), 0, jnp.maximum(room, 0))
    shifted = jax.random.randint(jax.random.fold_in(own, 4), (amount // 2,), 0, 1 << 20) % (room + 1)
    tallies = tallies.at[giver].add(-shifted).at[taker].add(shifted)
    members = jnp.searchsorted(jnp.cumsum(tallies), jnp.arange(rows * top), side="right").astype(jnp.int32)
    listing = members.reshape(top, rows).T
    listing = listing[jax.random.permutation(jax.random.fold_in(own, 1), rows)]
    rotation = jax.random.randint(jax.random.fold_in(own, 2), (rows, 1), 0, top)
    return jnp.take_along_axis(listing, (jnp.arange(top)[None, :] + rotation) % top, axis=1)


def portions_of(count, total, reach, skew, full):
    weights = [(1 << 20) // math.isqrt(standing ** skew) + 1 for standing in range(1, count + 1)]
    largest = reach if full else min(reach, max(-(-total // count), total * weights[0] // sum(weights)))
    least = 1 if total - largest >= count - 1 else 0
    given, surplus = [largest] + [least] * (count - 1), total - largest - least * (count - 1)
    while surplus > 0:
        free = [i for i in range(1, count) if given[i] < largest] or [i for i in range(1, count) if given[i] < reach]
        mass, left = sum([weights[i] for i in free]), surplus
        for i in free:
            extra = min(reach - given[i], max(1, left * weights[i] // mass), surplus)
            given[i] = given[i] + extra
            surplus = surplus - extra
    return np.array(given)


def bell_draw(own_key, dims, width, most, cuts=(), kind=jnp.bfloat16):
    drawn = jax.random.normal(own_key, dims, jnp.float32) * width
    if len(cuts) > 0:
        drawn = levels(own_key, dims, cuts, -0.22, 0.18) * drawn
    return jnp.clip(drawn, min=-most, max=most).astype(kind)


def setup_inputs(seed: int = 0) -> dict:
    arg_keys = jax.random.split(jax.random.key(seed), 21)
    stream = bell_draw(arg_keys[0], (TOKEN_COUNT, D), 1.0, 6.0, ((0, 256),))
    queries = bell_draw(arg_keys[1], (TOKEN_COUNT, HEAD_TOTAL * KEY_CHANNELS), 1.0, 6.0, ((0, 64), (1, 4)))
    key_rows = bell_draw(arg_keys[2], (TOKEN_COUNT, HEAD_TOTAL * KEY_CHANNELS), 1.0, 6.0, ((0, 64), (1, 4)))
    values = bell_draw(arg_keys[3], (TOKEN_COUNT, HV), 1.0, 6.0, ((0, 64), (1, 4)))
    out_gate = bell_draw(arg_keys[4], (TOKEN_COUNT, HV), 1.0, 6.0, ((0, 64), (1, 4)))
    fwd_decay = draw_fwd_decay(jax.random.fold_in(arg_keys[20], 71), 0)
    bwd_decay = draw_bwd_decay(jax.random.fold_in(arg_keys[20], 71), 0)
    head_gain = jnp.clip(1.0 + 0.18 * jax.random.normal(arg_keys[7], (HV,), jnp.float32), 0.1, 1.9)
    out_proj = bell_draw(arg_keys[8], (HV, D), HV ** -0.5, 0.1875)
    mix_gain = jnp.clip(1.0 + 0.18 * jax.random.normal(arg_keys[9], (D,), jnp.float32), 0.1, 1.9)
    ffn_gain = jnp.clip(1.0 + 0.18 * jax.random.normal(arg_keys[10], (D,), jnp.float32), 0.1, 1.9)
    moe_gain = jnp.clip(1.0 + 0.18 * jax.random.normal(arg_keys[11], (D,), jnp.float32), 0.1, 1.9)
    routes_keys = jax.random.split(jax.random.fold_in(arg_keys[12], 1), TOKEN_COUNT // TOK_DEV)
    routes_turns = jax.random.permutation(jax.random.fold_in(arg_keys[12], 3), TOKEN_COUNT // TOK_DEV)
    routes = jax.vmap(lambda own, number: deal_out(jax.random.fold_in(arg_keys[12], 2), own, number, TOK_DEV, EXPERTS, TOPK, CAP, 1))(routes_keys, routes_turns).reshape((TOKEN_COUNT, TOPK))
    route_weight = jnp.clip(jnp.exp(math.log(2.5) - 2.3025851 * jax.random.uniform(arg_keys[13], (TOKEN_COUNT, TOPK), jnp.float32) ** levels(arg_keys[13], (TOKEN_COUNT, TOPK), ((0, 256),), -0.2, 0.2)), 0.25, 2.5)
    expert_gate = bell_draw(arg_keys[14], (EXPERTS, D, FE), D ** -0.5, 0.125, ((0, 64), (2, 4)))
    expert_up = bell_draw(arg_keys[15], (EXPERTS, D, FE), D ** -0.5, 0.125, ((0, 64), (2, 4)))
    expert_down = bell_draw(arg_keys[16], (EXPERTS, FE, D), FE ** -0.5, 0.1875, ((0, 64), (1, 4)))
    shared_gate = bell_draw(arg_keys[17], (D, SH), D ** -0.5, 0.125, ((1, 4),))
    shared_up = bell_draw(arg_keys[18], (D, SH), D ** -0.5, 0.125, ((1, 4),))
    shared_down = bell_draw(arg_keys[19], (SH, D), SH ** -0.5, 0.25, ((0, 4),))
    return {"stream": stream, "queries": queries, "key_rows": key_rows, "values": values, "out_gate": out_gate, "fwd_decay": fwd_decay, "bwd_decay": bwd_decay, "head_gain": head_gain, "out_proj": out_proj, "mix_gain": mix_gain, "ffn_gain": ffn_gain, "moe_gain": moe_gain, "routes": routes, "route_weight": route_weight, "expert_gate": expert_gate, "expert_up": expert_up, "expert_down": expert_down, "shared_gate": shared_gate, "shared_up": shared_up, "shared_down": shared_down}


EPS = 1e-06
GATE_NORM = 16.0
ROPE_BASE = 10000.0
TOP_PRECISION = lax.Precision.HIGHEST

def normalize(tensor):
    return tensor * lax.rsqrt(lax.optimization_barrier(jnp.mean(tensor * tensor, axis=-1, keepdims=True)) + EPS)

def rotate(tensor, positions):
    half_width = tensor.shape[-1] // 2
    frequency = ROPE_BASE ** (-jnp.arange(half_width, dtype=jnp.float32) / half_width)
    angles = positions[:, None] * frequency[None, :]
    cosine = jnp.cos(angles)[:, None, :]
    sine_part = jnp.sin(angles)[:, None, :]
    front_half = tensor[..., :half_width]
    back_half = tensor[..., half_width:]
    return jnp.concatenate([front_half * cosine - back_half * sine_part, front_half * sine_part + back_half * cosine], axis=-1)

def blockwise(query_rows, key_data, value_matrix, log_decay, start_state):
    length, head_count, key_width = query_rows.shape
    value_width = value_matrix.shape[-1]
    block_count = length // BLK
    query_blocks = query_rows.reshape(block_count, BLK, head_count, key_width)
    key_blocks = key_data.reshape(block_count, BLK, head_count, key_width)
    value_blocks = value_matrix.reshape(block_count, BLK, head_count, value_width)
    cumul = jnp.cumsum(log_decay.reshape(block_count, BLK, head_count, key_width), axis=1)
    middle = cumul[:, BLK // 2 - 1:BLK // 2]
    query_scaled = query_blocks * jnp.exp(cumul - middle)
    key_scaled = key_blocks * jnp.exp(middle - cumul)
    scores = jnp.einsum('nthk,nshk->nhts', query_scaled, key_scaled, precision=TOP_PRECISION)
    lower_mask = jnp.arange(BLK)[:, None] >= jnp.arange(BLK)[None, :]
    scores = jnp.where(lower_mask, scores, 0.0)
    within = jnp.einsum('nhts,nshv->nthv', scores, value_blocks, precision=TOP_PRECISION)
    last_cumul = cumul[:, -1:]
    query_in = query_blocks * jnp.exp(cumul)
    key_out = key_blocks * jnp.exp(last_cumul - cumul)
    block_decay = jnp.exp(last_cumul[:, 0])

    def advance(carried_state, pieces):
        query_segment, key_segment, value_segment, decay_segment = pieces
        across_blocks = jnp.einsum('asu,sun->asn', query_segment, carried_state, precision=TOP_PRECISION)
        carried_state = carried_state * decay_segment[:, :, None] + jnp.einsum('jco,jcm->com', key_segment, value_segment, precision=TOP_PRECISION)
        return (carried_state, across_blocks)
    final_state, across_blocks = lax.scan(advance, start_state, (query_in, key_out, value_blocks, block_decay))
    return ((within + across_blocks).reshape(length, head_count, value_width), final_state)

def reference(stream, queries, key_rows, values, out_gate, fwd_decay, bwd_decay, head_gain, out_proj, mix_gain, ffn_gain, moe_gain, routes, route_weight, expert_gate, expert_up, expert_down, shared_gate, shared_up, shared_down):
    positions = jnp.arange(TOKEN_COUNT, dtype=jnp.int32).astype(jnp.float32)
    query_rows = rotate(queries.astype(jnp.float32).reshape(TOKEN_COUNT, HEAD_TOTAL, KEY_CHANNELS) * KEY_CHANNELS ** (-0.5), positions)
    key_data = rotate(key_rows.astype(jnp.float32).reshape(TOKEN_COUNT, HEAD_TOTAL, KEY_CHANNELS), positions)
    value_matrix = values.astype(jnp.float32).reshape(TOKEN_COUNT, HEAD_TOTAL, DV)
    fwd_log = jax.nn.log_sigmoid(fwd_decay).reshape(TOKEN_COUNT, HEAD_TOTAL, KEY_CHANNELS) / GATE_NORM
    bwd_log = jax.nn.log_sigmoid(bwd_decay).reshape(TOKEN_COUNT, HEAD_TOTAL, KEY_CHANNELS) / GATE_NORM
    zero_state = jnp.zeros((HEAD_TOTAL, KEY_CHANNELS, DV), jnp.float32)
    fwd_out, _ = blockwise(query_rows, key_data, value_matrix, fwd_log, zero_state)
    bwd_out, _ = blockwise(query_rows[::-1], key_data[::-1], value_matrix[::-1], bwd_log[::-1], zero_state)
    combined = normalize(fwd_out + bwd_out[::-1]) * head_gain.reshape(HEAD_TOTAL, DV)
    mixed_out = (combined.reshape(TOKEN_COUNT, HV) * jax.nn.silu(out_gate.astype(jnp.float32))).astype(jnp.bfloat16)
    projected = jnp.dot(mixed_out, out_proj, preferred_element_type=jnp.float32)
    residual = (stream.astype(jnp.float32) + normalize(projected) * mix_gain).astype(jnp.bfloat16)
    normed = (normalize(residual.astype(jnp.float32)) * ffn_gain).astype(jnp.bfloat16)
    shared_hidden = (jax.nn.silu(jnp.dot(normed, shared_gate, preferred_element_type=jnp.float32)) * jnp.dot(normed, shared_up, preferred_element_type=jnp.float32)).astype(jnp.bfloat16)
    group_width = SH // PARTS_SIZE
    shared_out = jnp.zeros((TOKEN_COUNT, D), jnp.float32)
    for quarter in range(PARTS_SIZE):
        piece = jnp.dot(shared_hidden[:, quarter * group_width:(quarter + 1) * group_width], shared_down[quarter * group_width:(quarter + 1) * group_width], preferred_element_type=jnp.float32)
        shared_out = shared_out + lax.optimization_barrier(piece.astype(jnp.bfloat16)).astype(jnp.float32)
    row_block = 256
    flat_ids = routes.reshape(-1)
    grand_total = flat_ids.shape[0]
    token_index = jnp.arange(grand_total, dtype=jnp.int32) // TOPK
    sort_order = jnp.argsort(flat_ids, stable=True)
    sorted_expert = flat_ids[sort_order]
    sorted_token = token_index[sort_order]
    sorted_weight = route_weight.reshape(-1)[sort_order]
    counts = lax.optimization_barrier(jnp.sum((flat_ids[:, None] == jnp.arange(EXPERTS, dtype=jnp.int32)[None, :]).astype(jnp.int32), axis=0))
    starts = jnp.cumsum(counts) - counts
    padded = (counts + row_block - 1) // row_block * row_block
    block_ends = jnp.cumsum(padded)
    padded_starts = block_ends - padded
    position = (padded_starts[sorted_expert] + jnp.arange(grand_total, dtype=jnp.int32) - starts[sorted_expert]).astype(jnp.int32)
    block_total = -(-(grand_total + EXPERTS * (row_block - 1)) // row_block)
    slot_token = jnp.zeros((block_total * row_block,), jnp.int32).at[position].set(sorted_token)
    slot_weight = jnp.zeros((block_total * row_block,), jnp.float32).at[position].set(sorted_weight)
    block_expert = jnp.minimum(jnp.searchsorted(block_ends, jnp.arange(block_total, dtype=jnp.int32) * row_block, side='right'), EXPERTS - 1).astype(jnp.int32)
    expert_width = FE // PARTS_SIZE

    def add_block(totals, block_item):
        token_ids, slot_wts, expert = block_item
        row_data = normed[token_ids]
        gate_mat = lax.dynamic_index_in_dim(expert_gate, expert, 0, keepdims=False)
        up_mat = lax.dynamic_index_in_dim(expert_up, expert, 0, keepdims=False)
        down_mat = lax.dynamic_index_in_dim(expert_down, expert, 0, keepdims=False)
        hidden = (jax.nn.silu(jnp.dot(row_data, gate_mat, preferred_element_type=jnp.float32)) * jnp.dot(row_data, up_mat, preferred_element_type=jnp.float32)).astype(jnp.bfloat16)
        quarter_sums = jnp.einsum('rqf,qfd->qrd', hidden.astype(jnp.float32).reshape(row_block, PARTS_SIZE, expert_width), down_mat.astype(jnp.float32).reshape(PARTS_SIZE, expert_width, D), precision=TOP_PRECISION)
        rounded = lax.optimization_barrier(quarter_sums.astype(jnp.bfloat16)).astype(jnp.float32)
        result = lax.optimization_barrier(lax.optimization_barrier(jnp.sum(rounded, axis=0)).astype(jnp.bfloat16)).astype(jnp.float32)
        return (totals.at[token_ids].add(result * slot_wts[:, None]), None)
    routed_sum, _ = lax.scan(add_block, jnp.zeros((TOKEN_COUNT, D), jnp.float32), (slot_token.reshape(block_total, row_block), slot_weight.reshape(block_total, row_block), block_expert))
    mixture = shared_out + routed_sum
    return (residual.astype(jnp.float32) + normalize(mixture) * moe_gain).astype(jnp.bfloat16)
```

```python
import functools

import jax
import jax.numpy as jnp
import numpy as np
from jax import lax
from jax.experimental import pallas as pl
from jax.experimental.pallas import tpu as pltpu
from jax.sharding import Mesh
from jax.sharding import PartitionSpec as P

KEY_CHANNELS = 64
DV = 128
BLK = 128
TOPK = 2
CAP = 6
Z, XC, TP = 8, 8, 4
SP = ("sp_0", "sp_1", "sp_2")
PLANE = ("sp_1", "sp_2")
SP_TP = ("sp_0", "sp_1", "sp_2", "tp")
SPAN = 512
TOK = 128
D = 2048
EXPERTS = 64
SLOTS = EXPERTS * CAP
LANES = 128
COLS = D // LANES
MSG = 272

EPS = 1e-06
GATE_NORM = 16.0
ROPE_BASE = 10000.0
F32 = jnp.float32
BF16 = jnp.bfloat16
HIGH = lax.Precision.HIGHEST
NT = (((1,), (1,)), ((), ()))
TN = (((0,), (0,)), ((), ()))
VMEM_LIMIT = 60 * 1024 * 1024


def rope_tables():
    half = KEY_CHANNELS // 2
    frequency = ROPE_BASE ** (-np.arange(half, dtype=np.float64) / half)
    lanes = np.tile(frequency, LANES // half)
    sign = np.tile(np.concatenate([-np.ones(half), np.ones(half)]), LANES // KEY_CHANNELS)
    inner = np.arange(BLK)[:, None] * lanes[None, :]
    local = np.stack([np.cos(inner), np.sin(inner) * sign, np.sin(inner), np.cos(inner) * sign])
    blocks = (np.arange(Z * XC * SPAN // BLK) * BLK)[:, None] * lanes[None, :]
    count = SPAN // BLK
    base = np.concatenate(
        [np.cos(blocks).reshape(-1, count, LANES), np.sin(blocks).reshape(-1, count, LANES)], axis=1
    )
    return local.astype(np.float32), base.astype(np.float32)


def dot(a, b, dims=(((1,), (0,)), ((), ())), precision=None):
    return lax.dot_general(a, b, dims, precision=precision, preferred_element_type=F32)


def iota(shape, axis):
    return lax.broadcasted_iota(jnp.int32, shape, axis)


def log_sigmoid(x):
    return jnp.minimum(x, 0.0) - jnp.log1p(jnp.exp(-jnp.abs(x)))


def spread(state, low):
    return jnp.concatenate([jnp.where(low, state, 0.0), jnp.where(low, 0.0, state)], axis=0)


def split_rows(rows):
    pieces = []
    for row in rows:
        high = row.astype(BF16)
        pieces += [high.astype(F32), row - high.astype(F32)]
    row_id = iota((16, LANES), 0)
    out = jnp.zeros((16, LANES), F32)
    for i, piece in enumerate(pieces):
        out = jnp.where(row_id == i, piece, out)
    return out


def attention_kernel(
    q_ref, k_ref, v_ref, fd_ref, bd_ref, local_ref, base_ref, routes_ref,
    part_ref, qdev_ref, msg_ref, slots_ref, within_ref, qin_ref,
):
    count = SPAN // BLK
    lane = iota((BLK, LANES), 1)
    low = lane < KEY_CHANNELS
    front = lane % KEY_CHANNELS < KEY_CHANNELS // 2
    row, col = iota((BLK, BLK), 0), iota((BLK, BLK), 1)
    tri_f = (row >= col).astype(F32)
    tri_b = (row <= col).astype(F32)
    row2, col2 = iota((BLK, 2 * BLK), 0), iota((BLK, 2 * BLK), 1) % BLK
    wide_low = iota((BLK, 2 * DV), 1) < DV

    def rotate(u, cosine, signed_sine):
        swapped = jnp.where(
            front,
            pltpu.roll(u, LANES - KEY_CHANNELS // 2, 1),
            pltpu.roll(u, KEY_CHANNELS // 2, 1),
        )
        return u * cosine + swapped * signed_sine

    updates_f, updates_b, last_f, last_b = [], [], [], []
    for n in range(count):
        rows = pl.ds(n * BLK, BLK)
        base_cos = base_ref[n : n + 1, :]
        base_sin = base_ref[count + n : count + n + 1, :]
        cosine = base_cos * local_ref[0] - base_sin * local_ref[2]
        signed_sine = base_sin * local_ref[3] + base_cos * local_ref[1]
        q = rotate(q_ref[rows, :].astype(F32) * KEY_CHANNELS ** (-0.5), cosine, signed_sine)
        k = rotate(k_ref[rows, :].astype(F32), cosine, signed_sine)
        v = v_ref[rows, :].astype(F32)
        v_bd = jnp.concatenate(
            [jnp.where(wide_low, v, 0.0), jnp.where(wide_low, 0.0, v)], axis=0
        ).astype(BF16)
        scores = jnp.zeros((BLK, 2 * BLK), F32)
        for forward in (True, False):
            log = log_sigmoid((fd_ref if forward else bd_ref)[rows, :]) * (1.0 / GATE_NORM)
            cumul = dot(tri_f if forward else tri_b, log, precision=HIGH)
            middle = cumul[BLK // 2 - 1 : BLK // 2, :] if forward else cumul[BLK // 2 : BLK // 2 + 1, :]
            total = cumul[BLK - 1 : BLK, :] if forward else cumul[0:1, :]
            offset = cumul - middle
            q_scaled = q * jnp.exp(offset)
            k_scaled = k * jnp.exp(-offset)
            q_in = q_scaled * jnp.exp(middle)
            k_out = k_scaled * jnp.exp(total - middle)
            both = dot(q_scaled.astype(BF16), spread(k_scaled, low).astype(BF16), NT)
            reach = row2 >= col2 if forward else row2 <= col2
            scores = scores + jnp.where(reach, both, 0.0)
            product = dot(v.astype(BF16), k_out.astype(BF16), TN)
            update = jnp.where(low, product[:DV], product[DV:])
            (updates_f if forward else updates_b).append(update)
            (last_f if forward else last_b).append(total)
            qin_ref[rows, pl.ds(0 if forward else LANES, LANES)] = q_in
        within_ref[rows, :] = dot(scores.astype(BF16), v_bd)

    zero_row = jnp.zeros((1, LANES), F32)
    states_f, states_b = [jnp.zeros((DV, LANES), F32)], [jnp.zeros((DV, LANES), F32)]
    sums_f, sums_b = [zero_row], [zero_row]
    for n in range(count):
        states_f.append(states_f[-1] * jnp.exp(last_f[n]) + updates_f[n])
        sums_f.append(sums_f[-1] + last_f[n])
        m = count - 1 - n
        states_b.append(states_b[-1] * jnp.exp(last_b[m]) + updates_b[m])
        sums_b.append(sums_b[-1] + last_b[m])
    for n in range(count):
        m = count - 1 - n
        rows = pl.ds(n * BLK, BLK)
        q_in = qin_ref[rows, :]
        carried = jnp.concatenate([spread(states_f[n], low), spread(states_b[m], low)], axis=1)
        part_ref[rows, :] = within_ref[rows, :] + dot(q_in.astype(BF16), carried.astype(BF16), NT)
        reach = jnp.exp(jnp.concatenate([sums_f[n], sums_b[m]], axis=1))
        qdev_ref[rows, :] = (q_in * reach).astype(BF16)
    final_f, final_b = states_f[count].astype(BF16), states_b[count].astype(BF16)
    sums = split_rows([sums_f[count], sums_b[count]]).astype(BF16)
    for j in range(XC):
        msg_ref[j, pl.ds(0, DV), :] = final_f
        msg_ref[j, pl.ds(DV, DV), :] = final_b
        msg_ref[j, pl.ds(2 * DV, 16), :] = sums

    expert = iota((TOK, EXPERTS), 1)
    picks = [routes_ref[:, k : k + 1] == expert for k in range(TOPK)]
    chosen = jnp.zeros((TOK, EXPERTS), F32)
    for pick in picks:
        chosen = chosen + pick.astype(F32)
    strict = (row > col).astype(BF16)
    before = dot(strict, chosen.astype(BF16))
    place = before + (CAP * expert).astype(F32)
    column = iota((TOK, TOPK), 1)
    slots = jnp.zeros((TOK, TOPK), F32)
    for k, pick in enumerate(picks):
        found = jnp.sum(jnp.where(pick, place, 0.0), axis=1, keepdims=True)
        slots = jnp.where(column == k, found, slots)
    slots_ref[...] = slots.astype(jnp.int32)


def compose_gathered(own, gathered_ref, length):
    results = []
    for forward in (True, False):
        start, at = (0, 2 * DV) if forward else (DV, 2 * DV + 2)
        state, logs = jnp.zeros((DV, LANES), F32), jnp.zeros((1, LANES), F32)
        inner, inner_logs = state, logs
        for step in range(length):
            k = step if forward else length - 1 - step
            here = own == k
            inner = jnp.where(here, state, inner)
            inner_logs = jnp.where(here, logs, inner_logs)
            tail = gathered_ref[k, pl.ds(2 * DV, 16), :].astype(F32)
            first = at - 2 * DV
            log = tail[first : first + 1, :] + tail[first + 1 : first + 2, :]
            state = state * jnp.exp(log) + gathered_ref[k, pl.ds(start, DV), :].astype(F32)
            logs = logs + log
        results.append((state, logs, inner, inner_logs))
    return results


def plane_kernel(own_ref, gathered_ref, inner_ref, logs_ref, msg_ref):
    forward, backward = compose_gathered(own_ref[0], gathered_ref, XC)
    inner_ref[0] = forward[2]
    inner_ref[1] = backward[2]
    row_id = iota((8, LANES), 0)
    logs_ref[...] = jnp.where(row_id == 0, forward[3], jnp.where(row_id == 1, backward[3], 0.0))
    total_f, total_b = forward[0].astype(BF16), backward[0].astype(BF16)
    sums = split_rows([forward[1], backward[1]]).astype(BF16)
    for j in range(Z):
        msg_ref[j, pl.ds(0, DV), :] = total_f
        msg_ref[j, pl.ds(DV, DV), :] = total_b
        msg_ref[j, pl.ds(2 * DV, 16), :] = sums


def readout_kernel(
    own_ref, gathered_ref, inner_ref, logs_ref, part_ref, qdev_ref, gate_ref, gain_ref, out_ref
):
    forward, backward = compose_gathered(own_ref[0], gathered_ref, Z)
    low = iota((DV, LANES), 1) < KEY_CHANNELS
    carry_f = inner_ref[0] + forward[2] * jnp.exp(logs_ref[0:1, :])
    carry_b = inner_ref[1] + backward[2] * jnp.exp(logs_ref[1:2, :])
    carried = jnp.concatenate([spread(carry_f, low), spread(carry_b, low)], axis=1).astype(BF16)
    for n in range(TP):
        rows = pl.ds(n * TOK, TOK)
        attended = part_ref[rows, :] + dot(qdev_ref[rows, :], carried, NT)
        heads = []
        for h in range(2):
            head = attended[:, h * DV : (h + 1) * DV]
            heads.append(head * lax.rsqrt(jnp.mean(head * head, axis=-1, keepdims=True) + EPS))
        gate = gate_ref[rows, :].astype(F32)
        mixed = jnp.concatenate(heads, axis=1) * gain_ref[...] * (gate * jax.nn.sigmoid(gate))
        out_ref[n] = mixed.astype(BF16)


def normalize(x):
    return x * lax.rsqrt(jnp.mean(x * x, axis=-1, keepdims=True) + EPS)


def project_kernel(
    slots_ref, mixed_ref, weight_ref, stream_ref, mix_ref, ffn_ref,
    residual_ref, normed_ref, sent_ref, acc_ref, rows_ref,
):
    step = pl.program_id(0)
    product = dot(mixed_ref[0], weight_ref[...])

    @pl.when(step == 0)
    def _():
        acc_ref[...] = product
        sent_ref[...] = jnp.zeros_like(sent_ref)

    @pl.when(step > 0)
    def _():
        acc_ref[...] += product

    @pl.when(step == TP - 1)
    def _():
        projected = normalize(acc_ref[...]) * mix_ref[...]
        residual = (stream_ref[...].astype(F32) + projected).astype(BF16)
        residual_ref[...] = residual
        normed = (normalize(residual.astype(F32)) * ffn_ref[...]).astype(BF16)
        normed_ref[...] = normed
        wide = normed.astype(F32)
        for j in range(COLS):
            rows_ref[pl.ds(j, TOK, stride=COLS), :] = wide[:, j * LANES : (j + 1) * LANES]

        def place(t, carry):
            line = rows_ref[pl.ds(pl.multiple_of(t * COLS, COLS), COLS), :].astype(BF16)
            for k in range(TOPK):
                sent_ref[slots_ref[t * TOPK + k]] = line
            return carry

        lax.fori_loop(0, TOK, place, 0, unroll=8)


def hidden_of(rows, gate, up):
    a = dot(rows, gate)
    return (a * jax.nn.sigmoid(a) * dot(rows, up)).astype(BF16)


def expert_kernel(sent_ref, gate_ref, up_ref, down_ref, out_ref, lines_ref, rows_ref, acc_ref):
    step = pl.program_id(0)

    @pl.when(step == 0)
    def _():
        lines_ref[...] = sent_ref[...].astype(F32)
        for j in range(COLS):
            rows_ref[:, j * LANES : (j + 1) * LANES] = lines_ref[
                pl.ds(j, SLOTS, stride=COLS), :
            ].astype(BF16)

    product = dot(hidden_of(rows_ref[...], gate_ref[0], up_ref[0]), down_ref[0])

    @pl.when(step == 0)
    def _():
        acc_ref[...] = product

    @pl.when(step > 0)
    def _():
        acc_ref[...] += product

    @pl.when(step == TP - 1)
    def _():
        for j in range(COLS):
            lines_ref[pl.ds(j, SLOTS, stride=COLS), :] = acc_ref[:, j * LANES : (j + 1) * LANES]
        out_ref[...] = lines_ref[...].astype(BF16)


def shared_kernel(rows_ref, gate_ref, up_ref, down_ref, out_ref):
    step = pl.program_id(0)
    product = dot(hidden_of(rows_ref[...], gate_ref[0], up_ref[0]), down_ref[0])

    @pl.when(step == 0)
    def _():
        out_ref[...] = product

    @pl.when(step > 0)
    def _():
        out_ref[...] += product


def combine_kernel(
    slots_ref, weights_ref, back_ref, shared_ref, residual_ref, gain_ref, out_ref, lines_ref, mix_ref
):
    def gather(t, carry):
        line = jnp.zeros((COLS, LANES), F32)
        for k in range(TOPK):
            at = t * TOPK + k
            line = line + back_ref[slots_ref[at]].astype(F32) * weights_ref[at]
        lines_ref[pl.ds(pl.multiple_of(t * COLS, COLS), COLS), :] = line
        return carry

    lax.fori_loop(0, TOK, gather, 0, unroll=8)
    for j in range(COLS):
        columns = slice(j * LANES, (j + 1) * LANES)
        mix_ref[:, columns] = shared_ref[:, columns] + lines_ref[pl.ds(j, TOK, stride=COLS), :]
    out_ref[...] = (
        residual_ref[...].astype(F32) + normalize(mix_ref[...]) * gain_ref[...]
    ).astype(BF16)


def vmem():
    return pl.BlockSpec(memory_space=pltpu.VMEM)


def smem():
    return pl.BlockSpec(memory_space=pltpu.SMEM)


def params(**extra):
    return pltpu.CompilerParams(vmem_limit_bytes=VMEM_LIMIT, **extra)


def shape(dims, kind):
    return jax.ShapeDtypeStruct(dims, kind)


def cost(flops, moved):
    return pl.CostEstimate(flops=flops, bytes_accessed=moved, transcendentals=0)


def whole(dims):
    return pl.BlockSpec(dims, lambda i, *_: (0,) * len(dims))


def body(
    stream,
    queries,
    key_rows,
    values,
    out_gate,
    fwd_decay,
    bwd_decay,
    head_gain,
    out_proj,
    mix_gain,
    ffn_gain,
    moe_gain,
    routes,
    route_weight,
    expert_gate,
    expert_up,
    expert_down,
    shared_gate,
    shared_up,
    shared_down,
):
    gates = lax.all_gather(expert_gate[0], "tp", axis=0)
    ups = lax.all_gather(expert_up[0], "tp", axis=0)
    downs = lax.all_gather(expert_down[0], "tp", axis=0)
    shared_gates = lax.all_gather(shared_gate, "tp", axis=0)
    shared_ups = lax.all_gather(shared_up, "tp", axis=0)
    shared_downs = lax.all_gather(shared_down, "tp", axis=0)

    local, base = rope_tables()
    base_here = lax.dynamic_index_in_dim(jnp.asarray(base), lax.axis_index(SP), 0, keepdims=False)
    part, qdev, msg, slots = pl.pallas_call(
        attention_kernel,
        out_shape=(
            shape((SPAN, 2 * DV), F32),
            shape((SPAN, 2 * LANES), BF16),
            shape((XC, MSG, LANES), BF16),
            shape((TOK, TOPK), jnp.int32),
        ),
        in_specs=[vmem()] * 8,
        out_specs=(vmem(),) * 4,
        scratch_shapes=[pltpu.VMEM((SPAN, 2 * DV), F32), pltpu.VMEM((SPAN, 2 * LANES), F32)],
        compiler_params=params(),
        cost_estimate=cost(600_000_000, 4_000_000),
        name="attention",
    )(queries, key_rows, values, fwd_decay, bwd_decay, jnp.asarray(local), base_here, routes)
    flat_slots = slots.reshape(-1)

    in_plane = lax.all_to_all(msg, PLANE, split_axis=0, concat_axis=0, tiled=True)
    inner, logs, msg = pl.pallas_call(
        plane_kernel,
        out_shape=(
            shape((2, DV, LANES), F32),
            shape((8, LANES), F32),
            shape((Z, MSG, LANES), BF16),
        ),
        in_specs=[smem(), vmem()],
        out_specs=(vmem(),) * 3,
        compiler_params=params(),
        cost_estimate=cost(10_000_000, 1_000_000),
        name="plane",
    )(lax.axis_index(PLANE).astype(jnp.int32).reshape(1), in_plane)
    planes = lax.all_to_all(msg, "sp_0", split_axis=0, concat_axis=0, tiled=True)
    mixed = pl.pallas_call(
        readout_kernel,
        out_shape=shape((TP, TOK, 2 * DV), BF16),
        in_specs=[smem()] + [vmem()] * 7,
        out_specs=vmem(),
        compiler_params=params(),
        cost_estimate=cost(100_000_000, 3_000_000),
        name="readout",
    )(
        lax.axis_index("sp_0").astype(jnp.int32).reshape(1),
        planes, inner, logs, part, qdev, out_gate, head_gain.reshape(1, -1),
    )
    mixed = lax.all_to_all(mixed, "tp", split_axis=0, concat_axis=0, tiled=True)

    residual, normed, sent = pl.pallas_call(
        project_kernel,
        grid=(TP,),
        out_shape=(
            shape((TOK, D), BF16),
            shape((TOK, D), BF16),
            shape((SLOTS, COLS, LANES), BF16),
        ),
        in_specs=[
            smem(),
            pl.BlockSpec((1, TOK, 2 * DV), lambda i: (i, 0, 0)),
            pl.BlockSpec((2 * DV, D), lambda i: (i, 0)),
            whole((TOK, D)),
            whole((1, D)),
            whole((1, D)),
        ],
        out_specs=(whole((TOK, D)), whole((TOK, D)), whole((SLOTS, COLS, LANES))),
        scratch_shapes=[pltpu.VMEM((TOK, D), F32), pltpu.VMEM((TOK * COLS, LANES), F32)],
        compiler_params=params(dimension_semantics=("arbitrary",)),
        cost_estimate=cost(600_000_000, 8_000_000),
        name="project",
    )(flat_slots, mixed, out_proj, stream, mix_gain.reshape(1, -1), ffn_gain.reshape(1, -1))

    arrived = lax.all_to_all(
        sent.reshape(EXPERTS, CAP * COLS, LANES), SP, split_axis=0, concat_axis=0, tiled=True
    )
    width = gates.shape[-1]
    done = pl.pallas_call(
        expert_kernel,
        grid=(TP,),
        out_shape=shape((SLOTS * COLS, LANES), BF16),
        in_specs=[
            whole((SLOTS * COLS, LANES)),
            pl.BlockSpec((1, D, width), lambda i: (i, 0, 0)),
            pl.BlockSpec((1, D, width), lambda i: (i, 0, 0)),
            pl.BlockSpec((1, width, D), lambda i: (i, 0, 0)),
        ],
        out_specs=whole((SLOTS * COLS, LANES)),
        scratch_shapes=[
            pltpu.VMEM((SLOTS * COLS, LANES), F32),
            pltpu.VMEM((SLOTS, D), BF16),
            pltpu.VMEM((SLOTS, D), F32),
        ],
        compiler_params=params(dimension_semantics=("arbitrary",)),
        cost_estimate=cost(4_900_000_000, 16_000_000),
        name="experts",
    )(arrived.reshape(SLOTS * COLS, LANES), gates, ups, downs)
    back = lax.all_to_all(
        done.reshape(EXPERTS, CAP * COLS, LANES), SP, split_axis=0, concat_axis=0, tiled=True
    )
    shared_width = shared_gates.shape[-1]
    shared = pl.pallas_call(
        shared_kernel,
        grid=(TP,),
        out_shape=shape((TOK, D), F32),
        in_specs=[
            whole((TOK, D)),
            pl.BlockSpec((1, D, shared_width), lambda i: (i, 0, 0)),
            pl.BlockSpec((1, D, shared_width), lambda i: (i, 0, 0)),
            pl.BlockSpec((1, shared_width, D), lambda i: (i, 0, 0)),
        ],
        out_specs=whole((TOK, D)),
        compiler_params=params(dimension_semantics=("arbitrary",)),
        cost_estimate=cost(800_000_000, 8_000_000),
        name="shared",
    )(normed, shared_gates, shared_ups, shared_downs)
    return pl.pallas_call(
        combine_kernel,
        out_shape=shape((TOK, D), BF16),
        in_specs=[smem(), smem()] + [vmem()] * 4,
        out_specs=vmem(),
        scratch_shapes=[pltpu.VMEM((TOK * COLS, LANES), F32), pltpu.VMEM((TOK, D), F32)],
        compiler_params=params(),
        cost_estimate=cost(5_000_000, 4_000_000),
        name="combine",
    )(
        flat_slots, route_weight.reshape(-1), back.reshape(SLOTS, COLS, LANES),
        shared, residual, moe_gain.reshape(1, -1),
    )


def solution(mesh):
    finer = Mesh(mesh.devices.reshape(8, 4, 2, mesh.shape["tp"]), ("sp_0", "sp_1", "sp_2", "tp"))
    placed = (
        P(SP_TP, None),
        P(SP, "tp"),
        P(SP, "tp"),
        P(SP, "tp"),
        P(SP, "tp"),
        P(SP, "tp"),
        P(SP, "tp"),
        P("tp"),
        P(),
        P(),
        P(),
        P(),
        P(SP_TP, None),
        P(SP_TP, None),
        P(SP, None, "tp"),
        P(SP, None, "tp"),
        P(SP, "tp", None),
        P(None, "tp"),
        P(None, "tp"),
        P("tp", None),
    )
    return jax.shard_map(
        body, mesh=finer, in_specs=placed, out_specs=P(SP_TP, None), check_vma=False
    )
```

```python
import jax
import jax.numpy as jnp
import numpy as np
from jax import lax
from jax.experimental import pallas as pl
from jax.experimental.pallas import tpu as pltpu
from jax.sharding import Mesh
from jax.sharding import PartitionSpec as P


KEY_CHANNELS = 64
DV = 128
BLK = 128
TOPK = 2
CAP = 6
Z, XC, TP = 8, 8, 4
SP = ("sp_0", "sp_1", "sp_2")
PLANE = ("sp_1", "sp_2")
SP_TP = ("sp_0", "sp_1", "sp_2", "tp")
SPAN = 512
TOK = 128
D = 2048
EXPERTS = 64
SLOTS = EXPERTS * CAP
LANES = 128
COLS = D // LANES
CHUNK = 256
CHUNKS = D // CHUNK
MSG = 272
HALF_MSG = 144

EPS = 1e-06
GATE_NORM = 16.0
ROPE_BASE = 10000.0
F32 = jnp.float32
BF16 = jnp.bfloat16
HIGH = lax.Precision.HIGHEST
NT = (((1,), (1,)), ((), ()))
TN = (((0,), (0,)), ((), ()))
VMEM_LIMIT = 60 * 1024 * 1024


def rope_tables():
    half = KEY_CHANNELS // 2
    frequency = ROPE_BASE ** (-np.arange(half, dtype=np.float64) / half)
    lanes = np.tile(frequency, LANES // half)
    sign = np.tile(np.concatenate([-np.ones(half), np.ones(half)]), LANES // KEY_CHANNELS)
    inner = np.arange(BLK)[:, None] * lanes[None, :]
    local = np.stack([np.cos(inner), np.sin(inner) * sign, np.sin(inner), np.cos(inner) * sign])
    blocks = (np.arange(Z * XC * SPAN // BLK) * BLK)[:, None] * lanes[None, :]
    count = SPAN // BLK
    base = np.concatenate(
        [np.cos(blocks).reshape(-1, count, LANES), np.sin(blocks).reshape(-1, count, LANES)], axis=1
    )
    return local.astype(np.float32), base.astype(np.float32)


def dot(a, b, dims=(((1,), (0,)), ((), ())), precision=None):
    return lax.dot_general(a, b, dims, precision=precision, preferred_element_type=F32)


def iota(shape, axis):
    return lax.broadcasted_iota(jnp.int32, shape, axis)


def log_sigmoid(x):
    return jnp.minimum(x, 0.0) - jnp.log1p(jnp.exp(-jnp.abs(x)))


def spread(state, low):
    return jnp.concatenate([jnp.where(low, state, 0.0), jnp.where(low, 0.0, state)], axis=0)


def split_rows(rows):
    pieces = []
    for row in rows:
        high = row.astype(BF16)
        pieces += [high.astype(F32), row - high.astype(F32)]
    row_id = iota((16, LANES), 0)
    out = jnp.zeros((16, LANES), F32)
    for i, piece in enumerate(pieces):
        out = jnp.where(row_id == i, piece, out)
    return out


def attention_kernel(
    q_ref, k_ref, v_ref, fd_ref, bd_ref, local_ref, base_ref, routes_ref,
    part_ref, qdev_ref, msg_ref, slots_ref, within_ref, qin_ref,
):
    count = SPAN // BLK
    lane = iota((BLK, LANES), 1)
    low = lane < KEY_CHANNELS
    front = lane % KEY_CHANNELS < KEY_CHANNELS // 2
    row, col = iota((BLK, BLK), 0), iota((BLK, BLK), 1)
    tri_f = (row >= col).astype(F32)
    tri_b = (row <= col).astype(F32)
    row2, col2 = iota((BLK, 2 * BLK), 0), iota((BLK, 2 * BLK), 1) % BLK
    wide_low = iota((BLK, 2 * DV), 1) < DV

    def rotate(u, cosine, signed_sine):
        swapped = jnp.where(
            front,
            pltpu.roll(u, LANES - KEY_CHANNELS // 2, 1),
            pltpu.roll(u, KEY_CHANNELS // 2, 1),
        )
        return u * cosine + swapped * signed_sine

    updates_f, updates_b, last_f, last_b = [], [], [], []
    for n in range(count):
        rows = pl.ds(n * BLK, BLK)
        base_cos = base_ref[n : n + 1, :]
        base_sin = base_ref[count + n : count + n + 1, :]
        cosine = base_cos * local_ref[0] - base_sin * local_ref[2]
        signed_sine = base_sin * local_ref[3] + base_cos * local_ref[1]
        q = rotate(q_ref[rows, :].astype(F32) * KEY_CHANNELS ** (-0.5), cosine, signed_sine)
        k = rotate(k_ref[rows, :].astype(F32), cosine, signed_sine)
        v = v_ref[rows, :].astype(F32)
        v_bd = jnp.concatenate(
            [jnp.where(wide_low, v, 0.0), jnp.where(wide_low, 0.0, v)], axis=0
        ).astype(BF16)
        scores = jnp.zeros((BLK, 2 * BLK), F32)
        for forward in (True, False):
            log = log_sigmoid((fd_ref if forward else bd_ref)[rows, :]) * (1.0 / GATE_NORM)
            cumul = dot(tri_f if forward else tri_b, log, precision=HIGH)
            middle = cumul[BLK // 2 - 1 : BLK // 2, :] if forward else cumul[BLK // 2 : BLK // 2 + 1, :]
            total = cumul[BLK - 1 : BLK, :] if forward else cumul[0:1, :]
            offset = cumul - middle
            q_scaled = q * jnp.exp(offset)
            k_scaled = k * jnp.exp(-offset)
            q_in = q_scaled * jnp.exp(middle)
            k_out = k_scaled * jnp.exp(total - middle)
            both = dot(q_scaled.astype(BF16), spread(k_scaled, low).astype(BF16), NT)
            reach = row2 >= col2 if forward else row2 <= col2
            scores = scores + jnp.where(reach, both, 0.0)
            product = dot(v.astype(BF16), k_out.astype(BF16), TN)
            update = jnp.where(low, product[:DV], product[DV:])
            (updates_f if forward else updates_b).append(update)
            (last_f if forward else last_b).append(total)
            qin_ref[rows, pl.ds(0 if forward else LANES, LANES)] = q_in
        within_ref[rows, :] = dot(scores.astype(BF16), v_bd)

    zero_row = jnp.zeros((1, LANES), F32)
    states_f, states_b = [jnp.zeros((DV, LANES), F32)], [jnp.zeros((DV, LANES), F32)]
    sums_f, sums_b = [zero_row], [zero_row]
    for n in range(count):
        states_f.append(states_f[-1] * jnp.exp(last_f[n]) + updates_f[n])
        sums_f.append(sums_f[-1] + last_f[n])
        m = count - 1 - n
        states_b.append(states_b[-1] * jnp.exp(last_b[m]) + updates_b[m])
        sums_b.append(sums_b[-1] + last_b[m])
    for n in range(count):
        m = count - 1 - n
        rows = pl.ds(n * BLK, BLK)
        q_in = qin_ref[rows, :]
        carried = jnp.concatenate([spread(states_f[n], low), spread(states_b[m], low)], axis=1)
        part_ref[rows, :] = within_ref[rows, :] + dot(q_in.astype(BF16), carried.astype(BF16), NT)
        reach = jnp.exp(jnp.concatenate([sums_f[n], sums_b[m]], axis=1))
        qdev_ref[rows, :] = (q_in * reach).astype(BF16)
    final_f, final_b = states_f[count].astype(BF16), states_b[count].astype(BF16)
    sums = split_rows([sums_f[count], sums_b[count]]).astype(BF16)
    msg_ref[pl.ds(0, DV), :] = final_f
    msg_ref[pl.ds(DV, DV), :] = final_b
    msg_ref[pl.ds(2 * DV, 16), :] = sums

    expert = iota((TOK, EXPERTS), 1)
    picks = [routes_ref[:, k : k + 1] == expert for k in range(TOPK)]
    chosen = jnp.zeros((TOK, EXPERTS), F32)
    for pick in picks:
        chosen = chosen + pick.astype(F32)
    strict = (row > col).astype(BF16)
    before = dot(strict, chosen.astype(BF16))
    place = before + (CAP * expert).astype(F32)
    column = iota((TOK, TOPK), 1)
    slots = jnp.zeros((TOK, TOPK), F32)
    for k, pick in enumerate(picks):
        found = jnp.sum(jnp.where(pick, place, 0.0), axis=1, keepdims=True)
        slots = jnp.where(column == k, found, slots)
    slots_ref[...] = slots.astype(jnp.int32)


def compose_gathered(own, gathered_ref, length, shared_place=False):
    results = []
    for forward in (True, False):
        start, tail_at, first = (0, 2 * DV, 0) if forward else (DV, 2 * DV, 2)
        if shared_place:
            start, tail_at, first = 0, DV, 0
        state, logs = jnp.zeros((DV, LANES), F32), jnp.zeros((1, LANES), F32)
        inner, inner_logs = state, logs
        for step in range(length):
            k = step if forward else length - 1 - step
            here = own == k
            inner = jnp.where(here, state, inner)
            inner_logs = jnp.where(here, logs, inner_logs)
            tail = gathered_ref[k, pl.ds(tail_at, 16), :].astype(F32)
            log = tail[first : first + 1, :] + tail[first + 1 : first + 2, :]
            state = state * jnp.exp(log) + gathered_ref[k, pl.ds(start, DV), :].astype(F32)
            logs = logs + log
        results.append((state, logs, inner, inner_logs))
    return results


def plane_kernel(own_ref, gathered_ref, inner_ref, logs_ref, msg_ref):
    forward, backward = compose_gathered(own_ref[0], gathered_ref, XC)
    inner_ref[0] = forward[2]
    inner_ref[1] = backward[2]
    row_id = iota((8, LANES), 0)
    logs_ref[...] = jnp.where(row_id == 0, forward[3], jnp.where(row_id == 1, backward[3], 0.0))
    for j in range(Z):
        later = own_ref[1] < j
        msg_ref[j, pl.ds(0, DV), :] = jnp.where(later, forward[0], backward[0]).astype(BF16)
        logs = jnp.where(later, forward[1], backward[1])
        msg_ref[j, pl.ds(DV, 16), :] = split_rows([logs]).astype(BF16)


def readout_kernel(
    own_ref, gathered_ref, inner_ref, logs_ref, part_ref, qdev_ref, gate_ref, gain_ref, *out_refs
):
    forward, backward = compose_gathered(own_ref[1], gathered_ref, Z, shared_place=True)
    low = iota((DV, LANES), 1) < KEY_CHANNELS
    carry_f = inner_ref[0] + forward[2] * jnp.exp(logs_ref[0:1, :])
    carry_b = inner_ref[1] + backward[2] * jnp.exp(logs_ref[1:2, :])
    carried = jnp.concatenate([spread(carry_f, low), spread(carry_b, low)], axis=1).astype(BF16)
    for n in range(TP):
        rows = pl.ds(pl.multiple_of((own_ref[2] + n) % TP * TOK, TOK), TOK)
        attended = part_ref[rows, :] + dot(qdev_ref[rows, :], carried, NT)
        heads = []
        for h in range(2):
            head = attended[:, h * DV : (h + 1) * DV]
            heads.append(head * lax.rsqrt(jnp.mean(head * head, axis=-1, keepdims=True) + EPS))
        gate = gate_ref[rows, :].astype(F32)
        mixed = jnp.concatenate(heads, axis=1) * gain_ref[...] * (gate * jax.nn.sigmoid(gate))
        out_refs[n][...] = mixed.astype(BF16)


def normalize(x):
    return x * lax.rsqrt(jnp.mean(x * x, axis=-1, keepdims=True) + EPS)


def project_kernel(
    own_ref, slots_ref, mixed_0, mixed_1, mixed_2, mixed_3, weight_ref, stream_ref, mix_ref,
    ffn_ref, residual_ref, normed_ref, sent_ref, acc_ref, rows_ref,
):
    step = pl.program_id(0)

    @pl.when(step == 0)
    def _():
        acc_ref[...] = dot(mixed_0[...], weight_ref[...])
        sent_ref[...] = jnp.zeros_like(sent_ref)

    for n, mixed_ref in enumerate((mixed_1, mixed_2, mixed_3)):

        @pl.when(step == n + 1)
        def _(mixed_ref=mixed_ref):
            acc_ref[...] += dot(mixed_ref[...], weight_ref[...])

    @pl.when(step == TP - 1)
    def _():
        projected = normalize(acc_ref[...]) * mix_ref[...]
        residual = (stream_ref[...].astype(F32) + projected).astype(BF16)
        residual_ref[...] = residual
        normed = (normalize(residual.astype(F32)) * ffn_ref[...]).astype(BF16)
        normed_ref[...] = normed
        wide = normed.astype(F32)
        for j in range(COLS):
            rows_ref[pl.ds(j, TOK, stride=COLS), :] = wide[:, j * LANES : (j + 1) * LANES]

        def place(t, carry):
            line = rows_ref[pl.ds(pl.multiple_of(t * COLS, COLS), COLS), :].astype(BF16)
            for k in range(TOPK):
                sent_ref[slots_ref[t * TOPK + k]] = line
            return carry

        lax.fori_loop(0, TOK, place, 0, unroll=8)


def pack_shared_kernel(gate_ref, up_ref, down_ref, after_ref, out_ref):
    for i in range(CHUNKS):
        rows = pl.ds(i * CHUNK, CHUNK)
        out_ref[i, pl.ds(0, CHUNK), pl.ds(0, LANES)] = gate_ref[rows, :]
        out_ref[i, pl.ds(0, CHUNK), pl.ds(LANES, LANES)] = up_ref[rows, :]
        out_ref[i, pl.ds(CHUNK, LANES), :] = down_ref[:, rows]


def pack_shared(gate, up, down, after):
    return pl.pallas_call(
        pack_shared_kernel,
        out_shape=shape((CHUNKS, CHUNK + LANES, CHUNK), BF16),
        in_specs=[vmem()] * 3 + [anywhere()],
        out_specs=vmem(),
        compiler_params=params(),
        cost_estimate=cost(1_000_000, 3_200_000),
        name="pack_shared",
    )(gate, up, down, after)


def silu(x):
    return x * jax.nn.sigmoid(x)


def expert_kernel(*refs):
    sent_ref, gates, ups = refs[0], refs[1:5], refs[5:9]
    downs = refs[9:13]
    out_ref, lines_ref, rows_ref, acc_ref, gate_ref, up_ref, down_ref, sems = refs[13:]

    def pieces(n):
        return [
            pltpu.make_async_copy(gates[n], gate_ref.at[n], sems.at[0, n]),
            pltpu.make_async_copy(ups[n], up_ref.at[n], sems.at[1, n]),
            pltpu.make_async_copy(downs[n], down_ref.at[n], sems.at[2, n]),
        ]

    for n in range(TP):
        for piece in pieces(n):
            piece.start()
    lines_ref[...] = sent_ref[...].astype(F32)
    for j in range(COLS):
        rows_ref[:, j * LANES : (j + 1) * LANES] = lines_ref[
            pl.ds(j, SLOTS, stride=COLS), :
        ].astype(BF16)
    acc_ref[...] = jnp.zeros_like(acc_ref)

    def shard(n, carry):
        pltpu.make_async_copy(gates[0], gate_ref.at[n], sems.at[0, n]).wait()
        pltpu.make_async_copy(ups[0], up_ref.at[n], sems.at[1, n]).wait()
        rows = rows_ref[...]
        hidden = (silu(dot(rows, gate_ref[n])) * dot(rows, up_ref[n])).astype(BF16)
        pltpu.make_async_copy(downs[0], down_ref.at[n], sems.at[2, n]).wait()
        for j in range(CHUNKS):
            columns = pl.ds(j * CHUNK, CHUNK)
            acc_ref[:, columns] += dot(hidden, down_ref[n, :, columns])
        return carry

    lax.fori_loop(0, TP, shard, 0)
    for j in range(COLS):
        lines_ref[pl.ds(j, SLOTS, stride=COLS), :] = acc_ref[:, j * LANES : (j + 1) * LANES]
    out_ref[...] = lines_ref[...].astype(BF16)


def shared_kernel(*refs):
    rows_ref, shards, out_ref, weight_ref, sems = refs[0], refs[1:6], refs[6], refs[7], refs[8]
    half = CHUNKS // 2
    copies = [pltpu.make_async_copy(shards[n], weight_ref.at[n], sems.at[n]) for n in range(TP - 1)]
    copies += [
        pltpu.make_async_copy(
            shards[TP - 1 + n], weight_ref.at[TP - 1, pl.ds(n * half, half)], sems.at[TP - 1 + n]
        )
        for n in range(2)
    ]
    for copy in copies:
        copy.start()
    for n in range(TP):
        copies[n].wait()
        if n == TP - 1:
            copies[TP].wait()
        joint = jnp.zeros((TOK, 2 * LANES), F32)
        for i in range(CHUNKS):
            columns = pl.ds(i * CHUNK, CHUNK)
            joint = joint + dot(rows_ref[:, columns], weight_ref[n, i, 0:CHUNK, :])
        hidden = (silu(joint[:, :LANES]) * joint[:, LANES:]).astype(BF16)
        for i in range(CHUNKS):
            columns = pl.ds(i * CHUNK, CHUNK)
            product = dot(hidden, weight_ref[n, i, CHUNK:, :])
            if n == 0:
                out_ref[:, columns] = product
            else:
                out_ref[:, columns] += product


def combine_kernel(
    slots_ref, weights_ref, back_ref, shared_ref, residual_ref, gain_ref, out_ref, lines_ref, mix_ref
):
    def gather(t, carry):
        line = jnp.zeros((COLS, LANES), F32)
        for k in range(TOPK):
            at = t * TOPK + k
            line = line + back_ref[slots_ref[at]].astype(F32) * weights_ref[at]
        lines_ref[pl.ds(pl.multiple_of(t * COLS, COLS), COLS), :] = line
        return carry

    lax.fori_loop(0, TOK, gather, 0, unroll=8)
    for j in range(COLS):
        columns = slice(j * LANES, (j + 1) * LANES)
        mix_ref[:, columns] = shared_ref[:, columns] + lines_ref[pl.ds(j, TOK, stride=COLS), :]
    out_ref[...] = (
        residual_ref[...].astype(F32) + normalize(mix_ref[...]) * gain_ref[...]
    ).astype(BF16)


def vmem():
    return pl.BlockSpec(memory_space=pltpu.VMEM)


def anywhere():
    return pl.BlockSpec(memory_space=pl.ANY)


def shift(array, hops):
    return lax.ppermute(array, "tp", [(i, (i + hops) % TP) for i in range(TP)])


def smem():
    return pl.BlockSpec(memory_space=pltpu.SMEM)


def params(**extra):
    return pltpu.CompilerParams(vmem_limit_bytes=VMEM_LIMIT, **extra)


def shape(dims, kind):
    return jax.ShapeDtypeStruct(dims, kind)


def cost(flops, moved):
    return pl.CostEstimate(flops=flops, bytes_accessed=moved, transcendentals=0)


def whole(dims):
    return pl.BlockSpec(dims, lambda i, *_: (0,) * len(dims))


def body(
    stream,
    queries,
    key_rows,
    values,
    out_gate,
    fwd_decay,
    bwd_decay,
    head_gain,
    out_proj,
    mix_gain,
    ffn_gain,
    moe_gain,
    routes,
    route_weight,
    expert_gate,
    expert_up,
    expert_down,
    shared_gate,
    shared_up,
    shared_down,
):
    own = jnp.stack([lax.axis_index(axes) for axes in (PLANE, "sp_0", "tp", "sp_2")])
    own = own.astype(jnp.int32)
    gate, up, down = expert_gate[0], expert_up[0], expert_down[0]
    gate_left = shift(gate, 1)
    gate_right = shift(gate, -1)
    up_left = shift(up, 1)
    up_right = shift(up, -1)

    local, base = rope_tables()
    base_here = lax.dynamic_index_in_dim(jnp.asarray(base), lax.axis_index(SP), 0, keepdims=False)
    part, qdev, msg, slots = pl.pallas_call(
        attention_kernel,
        out_shape=(
            shape((SPAN, 2 * DV), F32),
            shape((SPAN, 2 * LANES), BF16),
            shape((MSG, LANES), BF16),
            shape((TOK, TOPK), jnp.int32),
        ),
        in_specs=[vmem()] * 8,
        out_specs=(vmem(),) * 4,
        scratch_shapes=[pltpu.VMEM((SPAN, 2 * DV), F32), pltpu.VMEM((SPAN, 2 * LANES), F32)],
        compiler_params=params(),
        cost_estimate=cost(600_000_000, 4_000_000),
        name="attention",
    )(queries, key_rows, values, fwd_decay, bwd_decay, jnp.asarray(local), base_here, routes)
    flat_slots = slots.reshape(-1)

    in_plane = lax.all_gather(msg, PLANE, axis=0)
    inner, logs, msg = pl.pallas_call(
        plane_kernel,
        out_shape=(
            shape((2, DV, LANES), F32),
            shape((8, LANES), F32),
            shape((Z, HALF_MSG, LANES), BF16),
        ),
        in_specs=[smem(), vmem()],
        out_specs=(vmem(),) * 3,
        compiler_params=params(),
        cost_estimate=cost(10_000_000, 1_000_000),
        name="plane",
    )(own, in_plane)
    planes = lax.all_to_all(msg, "sp_0", split_axis=0, concat_axis=0, tiled=True)
    mixed = pl.pallas_call(
        readout_kernel,
        out_shape=(shape((TOK, 2 * DV), BF16),) * TP,
        in_specs=[smem()] + [vmem()] * 7,
        out_specs=(vmem(),) * TP,
        compiler_params=params(),
        cost_estimate=cost(100_000_000, 3_000_000),
        name="readout",
    )(
        own, planes, inner, logs, part, qdev, out_gate, head_gain.reshape(1, -1),
    )
    mixed = [shift(piece, n) if n else piece for n, piece in enumerate(mixed)]

    down_left = shift(down, 1)
    down_right = shift(down, -1)
    gate_far = shift(gate_left, 1)
    up_far = shift(up_right, -1)
    down_far_1 = shift(down_left[: down.shape[0] // 2], 1)
    down_far_2 = shift(down_right[down.shape[0] // 2 :], -1)

    residual, normed, sent = pl.pallas_call(
        project_kernel,
        out_shape=(
            shape((TOK, D), BF16),
            shape((TOK, D), BF16),
            shape((SLOTS, COLS, LANES), BF16),
        ),
        grid_spec=pltpu.PrefetchScalarGridSpec(
            num_scalar_prefetch=2,
            grid=(TP,),
            in_specs=[whole((TOK, 2 * DV))] * TP
            + [
                pl.BlockSpec((2 * DV, D), lambda i, own, _: ((own[2] + TP - i) % TP, 0)),
                whole((TOK, D)),
                whole((1, D)),
                whole((1, D)),
            ],
            out_specs=(whole((TOK, D)), whole((TOK, D)), whole((SLOTS, COLS, LANES))),
            scratch_shapes=[pltpu.VMEM((TOK, D), F32), pltpu.VMEM((TOK * COLS, LANES), F32)],
        ),
        compiler_params=params(dimension_semantics=("arbitrary",)),
        cost_estimate=cost(600_000_000, 8_000_000),
        name="project",
    )(own, flat_slots, *mixed, out_proj, stream, mix_gain.reshape(1, -1), ffn_gain.reshape(1, -1))

    arrived = lax.all_to_all(
        sent.reshape(EXPERTS, CAP * COLS, LANES), SP, split_axis=0, concat_axis=0, tiled=True
    )
    width = gate.shape[1]
    down_far = jnp.concatenate([down_far_1, down_far_2], axis=0)
    done = pl.pallas_call(
        expert_kernel,
        out_shape=shape((SLOTS * COLS, LANES), BF16),
        in_specs=[vmem()] + [anywhere()] * 12,
        out_specs=vmem(),
        scratch_shapes=[
            pltpu.VMEM((SLOTS * COLS, LANES), F32),
            pltpu.VMEM((SLOTS, D), BF16),
            pltpu.VMEM((SLOTS, D), F32),
            pltpu.VMEM((TP, D, width), BF16),
            pltpu.VMEM((TP, D, width), BF16),
            pltpu.VMEM((TP, width, D), BF16),
            pltpu.SemaphoreType.DMA((3, TP)),
        ],
        compiler_params=params(),
        cost_estimate=cost(4_900_000_000, 16_000_000),
        name="experts",
    )(
        arrived.reshape(SLOTS * COLS, LANES),
        gate, gate_left, gate_right, gate_far,
        up, up_left, up_right, up_far,
        down, down_left, down_right, down_far,
    )
    back = lax.all_to_all(
        done.reshape(EXPERTS, CAP * COLS, LANES), SP, split_axis=0, concat_axis=0, tiled=True
    )
    packed = pack_shared(shared_gate, shared_up, shared_down, residual)
    half = CHUNKS // 2
    shared_left = shift(packed, 1)
    shared_right = shift(packed, -1)
    shared_far_1 = shift(shared_left[:half], 1)
    shared_far_2 = shift(shared_right[half:], -1)
    shared = pl.pallas_call(
        shared_kernel,
        out_shape=shape((TOK, D), F32),
        in_specs=[vmem()] + [anywhere()] * 5,
        out_specs=vmem(),
        scratch_shapes=[
            pltpu.VMEM((TP, *packed.shape), BF16),
            pltpu.SemaphoreType.DMA((TP + 1,)),
        ],
        compiler_params=params(),
        cost_estimate=cost(800_000_000, 8_000_000),
        name="shared",
    )(normed, packed, shared_left, shared_right, shared_far_1, shared_far_2)
    return pl.pallas_call(
        combine_kernel,
        out_shape=shape((TOK, D), BF16),
        in_specs=[smem(), smem()] + [vmem()] * 4,
        out_specs=vmem(),
        scratch_shapes=[pltpu.VMEM((TOK * COLS, LANES), F32), pltpu.VMEM((TOK, D), F32)],
        compiler_params=params(),
        cost_estimate=cost(5_000_000, 4_000_000),
        name="combine",
    )(
        flat_slots, route_weight.reshape(-1), back.reshape(SLOTS, COLS, LANES),
        shared, residual, moe_gain.reshape(1, -1),
    )


def solution(mesh):
    finer = Mesh(mesh.devices.reshape(8, 4, 2, mesh.shape["tp"]), ("sp_0", "sp_1", "sp_2", "tp"))
    placed = (
        P(SP_TP, None),
        P(SP, "tp"),
        P(SP, "tp"),
        P(SP, "tp"),
        P(SP, "tp"),
        P(SP, "tp"),
        P(SP, "tp"),
        P("tp"),
        P(),
        P(),
        P(),
        P(),
        P(SP_TP, None),
        P(SP_TP, None),
        P(SP, None, "tp"),
        P(SP, None, "tp"),
        P(SP, "tp", None),
        P(None, "tp"),
        P(None, "tp"),
        P("tp", None),
    )

    return jax.shard_map(
        body, mesh=finer, in_specs=placed, out_specs=P(SP_TP, None), check_vma=False
    )
```

```python
import jax
import jax.numpy as jnp
import numpy as np
from jax import lax
from jax.experimental import pallas as pl
from jax.experimental.pallas import tpu as pltpu
from jax.sharding import Mesh
from jax.sharding import PartitionSpec as P


KEY_CHANNELS = 64
DV = 128
BLK = 128
TOPK = 2
CAP = 6
Z, XC, TP = 8, 8, 4
SP = ("sp_0", "sp_1", "sp_2")
PLANE = ("sp_1", "sp_2")
SP_TP = ("sp_0", "sp_1", "sp_2", "tp")
SPAN = 512
TOK = 128
D = 2048
EXPERTS = 64
SLOTS = EXPERTS * CAP
LANES = 128
COLS = D // LANES
CHUNK = 256
PIECES = 4
CHUNKS = D // CHUNK
MSG = 272
HALF_MSG = 144

EPS = 1e-06
GATE_NORM = 16.0
ROPE_BASE = 10000.0
F32 = jnp.float32
BF16 = jnp.bfloat16
NT = (((1,), (1,)), ((), ()))
TN = (((0,), (0,)), ((), ()))


def rope_tables():
    half = KEY_CHANNELS // 2
    frequency = ROPE_BASE ** (-np.arange(half, dtype=np.float64) / half)
    lanes = np.tile(frequency, LANES // half)
    tables = []
    for count, step in ((BLK, 1), (SPAN // BLK, BLK), (Z * XC, SPAN)):
        angles = (np.arange(count) * step)[:, None] * lanes[None, :]
        tables.append(np.stack([np.cos(angles), np.sin(angles)], axis=0).astype(np.float32))
    return tables[0], tables[1].reshape(-1, LANES), tables[2].swapaxes(0, 1)


def dot(a, b, dims=(((1,), (0,)), ((), ()))):
    return lax.dot_general(a, b, dims, preferred_element_type=F32)


def iota(shape, axis):
    return lax.broadcasted_iota(jnp.int32, shape, axis)


def log_sigmoid(x):
    return jnp.minimum(x, 0.0) - jnp.log1p(jnp.exp(-jnp.abs(x)))


def spread(state, low):
    return jnp.concatenate([jnp.where(low, state, 0.0), jnp.where(low, 0.0, state)], axis=0)


def split_rows(rows):
    pieces = []
    for row in rows:
        high = row.astype(BF16)
        pieces += [high.astype(F32), row - high.astype(F32)]
    row_id = iota((16, LANES), 0)
    out = jnp.zeros((16, LANES), F32)
    for i, piece in enumerate(pieces):
        out = jnp.where(row_id == i, piece, out)
    return out


class Block:
    def __init__(self, own_ref, local_ref, block_ref, base_ref):
        self.count = SPAN // BLK
        lane = iota((BLK, LANES), 1)
        self.low = lane < KEY_CHANNELS
        self.front = lane % KEY_CHANNELS < KEY_CHANNELS // 2
        self.row, self.col = iota((BLK, BLK), 0), iota((BLK, BLK), 1)
        self.local, self.blocks = local_ref, block_ref
        self.base = base_ref[own_ref[1] * XC + own_ref[0]]

    def tables(self, n):
        def add(a, b):
            return a[0] * b[0] - a[1] * b[1], a[1] * b[0] + a[0] * b[1]

        span = self.base[0:1, :], self.base[1:2, :]
        m = self.count + n
        start = add(span, (self.blocks[n : n + 1, :], self.blocks[m : m + 1, :]))
        cosine, sine = add(start, (self.local[0], self.local[1]))
        return cosine, jnp.where(self.front, -sine, sine)

    def rotate(self, u, tables):
        swapped = jnp.where(
            self.front,
            pltpu.roll(u, LANES - KEY_CHANNELS // 2, 1),
            pltpu.roll(u, KEY_CHANNELS // 2, 1),
        )
        return u * tables[0] + swapped * tables[1]

    def decays(self, log_ref, forward):
        tri = (self.row >= self.col if forward else self.row <= self.col).astype(BF16)
        parts = []
        for n in range(self.count):
            log = log_sigmoid(log_ref[pl.ds(n * BLK, BLK), :]) * (1.0 / GATE_NORM)
            for _ in range(3):
                part = log.astype(BF16)
                parts.append(part)
                log = log - part.astype(F32)
        sums = dot(tri, jnp.concatenate(parts, axis=1))
        pieces = [sums[:, i * LANES : (i + 1) * LANES] for i in range(3 * self.count)]
        return [sum(pieces[3 * n + 1 : 3 * n + 3], pieces[3 * n]) for n in range(self.count)]


def states_kernel(
    own_ref, k_ref, v_ref, fd_ref, bd_ref, local_ref, block_ref, base_ref,
    msg_ref, key_ref, cumul_ref, states_ref,
):
    block = Block(own_ref, local_ref, block_ref, base_ref)
    count, low = block.count, block.low
    updates, lasts = ([], []), ([], [])
    decays = [block.decays(fd_ref, True), block.decays(bd_ref, False)]
    for n in range(count):
        rows = pl.ds(n * BLK, BLK)
        k = block.rotate(k_ref[rows, :].astype(F32), block.tables(n))
        key_ref[rows, :] = k
        v = v_ref[rows, :]
        for d in range(2):
            cumul = decays[d][n]
            end = BLK - 1 if d == 0 else 0
            total = cumul[end : end + 1, :]
            cumul_ref[d, rows, :] = cumul
            k_out = k * jnp.exp(total - cumul)
            product = dot(v, k_out.astype(BF16), TN)
            updates[d].append(jnp.where(low, product[:DV], product[DV:]))
            lasts[d].append(total)
    finals, sums = [], []
    for d in range(2):
        state, logs = jnp.zeros((DV, LANES), F32), jnp.zeros((1, LANES), F32)
        for n in range(count) if d == 0 else reversed(range(count)):
            states_ref[d, n] = state
            state = state * jnp.exp(lasts[d][n]) + updates[d][n]
            logs = logs + lasts[d][n]
        finals.append(state.astype(BF16))
        sums.append(logs)
    tail = split_rows(sums).astype(BF16)
    for j in range(XC):
        msg_ref[j, pl.ds(0, DV), :] = finals[0]
        msg_ref[j, pl.ds(DV, DV), :] = finals[1]
        msg_ref[j, pl.ds(2 * DV, 16), :] = tail


def attention_kernel(
    own_ref, q_ref, v_ref, key_ref, cumul_ref, states_ref, local_ref, block_ref, base_ref,
    routes_ref,
    part_ref, qdev_ref, slots_ref,
):
    block = Block(own_ref, local_ref, block_ref, base_ref)
    count, low, row, col = block.count, block.low, block.row, block.col
    row2, col2 = iota((BLK, 2 * BLK), 0), iota((BLK, 2 * BLK), 1) % BLK
    wide_low = iota((BLK, 2 * DV), 1) < DV
    zero_row = jnp.zeros((1, LANES), F32)
    lasts = [
        [cumul_ref[0, pl.ds(n * BLK + BLK - 1, 1), :] for n in range(count)],
        [cumul_ref[1, pl.ds(n * BLK, 1), :] for n in range(count)],
    ]
    for n in range(count):
        rows = pl.ds(n * BLK, BLK)
        scale = KEY_CHANNELS ** (-0.5)
        q = block.rotate(q_ref[rows, :].astype(F32) * scale, block.tables(n))
        k = key_ref[rows, :]
        v = v_ref[rows, :].astype(F32)
        v_bd = jnp.concatenate(
            [jnp.where(wide_low, v, 0.0), jnp.where(wide_low, 0.0, v)], axis=0
        ).astype(BF16)
        scores = jnp.zeros((BLK, 2 * BLK), F32)
        q_ins, carried, reaches = [], [], []
        for d in range(2):
            cumul = cumul_ref[d, rows, :]
            at = BLK // 2 - 1 if d == 0 else BLK // 2
            middle = cumul[at : at + 1, :]
            offset = cumul - middle
            q_scaled = q * jnp.exp(offset)
            k_scaled = k * jnp.exp(-offset)
            both = dot(q_scaled.astype(BF16), spread(k_scaled, low).astype(BF16), NT)
            reach = row2 >= col2 if d == 0 else row2 <= col2
            scores = scores + jnp.where(reach, both, 0.0)
            q_ins.append(q_scaled * jnp.exp(middle))
            carried.append(spread(states_ref[d, n], low))
            passed = range(n) if d == 0 else range(n + 1, count)
            reaches.append(sum((lasts[d][m] for m in passed), zero_row))
        q_in = jnp.concatenate(q_ins, axis=1)
        within = dot(scores.astype(BF16), v_bd)
        across = dot(q_in.astype(BF16), jnp.concatenate(carried, axis=1).astype(BF16), NT)
        part_ref[rows, :] = within + across
        qdev_ref[rows, :] = (q_in * jnp.exp(jnp.concatenate(reaches, axis=1))).astype(BF16)

    expert = iota((EXPERTS, TOK), 0)
    picks = [routes_ref[k : k + 1, :] == expert for k in range(TOPK)]
    chosen = jnp.zeros((EXPERTS, TOK), F32)
    for pick in picks:
        chosen = chosen + pick.astype(F32)
    strict = (row < col).astype(BF16)
    before = dot(chosen.astype(BF16), strict)
    place = before + (CAP * expert).astype(F32)
    for k, pick in enumerate(picks):
        found = jnp.sum(jnp.where(pick, place, 0.0), axis=0, keepdims=True)
        slots_ref[k : k + 1, :] = found.astype(jnp.int32)


def compose_gathered(own, gathered_ref, length, shared_place=False):
    results = []
    for forward in (True, False):
        start, tail_at, first = (0, 2 * DV, 0) if forward else (DV, 2 * DV, 2)
        if shared_place:
            start, tail_at, first = 0, DV, 0
        state, logs = jnp.zeros((DV, LANES), F32), jnp.zeros((1, LANES), F32)
        inner, inner_logs = state, logs
        for step in range(length):
            k = step if forward else length - 1 - step
            here = own == k
            inner = jnp.where(here, state, inner)
            inner_logs = jnp.where(here, logs, inner_logs)
            tail = gathered_ref[k, pl.ds(tail_at, 16), :].astype(F32)
            log = tail[first : first + 1, :] + tail[first + 1 : first + 2, :]
            state = state * jnp.exp(log) + gathered_ref[k, pl.ds(start, DV), :].astype(F32)
            logs = logs + log
        results.append((state, logs, inner, inner_logs))
    return results


def plane_kernel(own_ref, gathered_ref, inner_ref, logs_ref, msg_ref):
    forward, backward = compose_gathered(own_ref[0], gathered_ref, XC)
    inner_ref[0] = forward[2]
    inner_ref[1] = backward[2]
    row_id = iota((8, LANES), 0)
    logs_ref[...] = jnp.where(row_id == 0, forward[3], jnp.where(row_id == 1, backward[3], 0.0))
    for j in range(Z):
        later = own_ref[1] < j
        msg_ref[j, pl.ds(0, DV), :] = jnp.where(later, forward[0], backward[0]).astype(BF16)
        logs = jnp.where(later, forward[1], backward[1])
        msg_ref[j, pl.ds(DV, 16), :] = split_rows([logs]).astype(BF16)


def readout_kernel(
    own_ref, gathered_ref, inner_ref, logs_ref, part_ref, qdev_ref, gate_ref, gain_ref, *out_refs
):
    forward, backward = compose_gathered(own_ref[1], gathered_ref, Z, shared_place=True)
    low = iota((DV, LANES), 1) < KEY_CHANNELS
    carry_f = inner_ref[0] + forward[2] * jnp.exp(logs_ref[0:1, :])
    carry_b = inner_ref[1] + backward[2] * jnp.exp(logs_ref[1:2, :])
    carried = jnp.concatenate([spread(carry_f, low), spread(carry_b, low)], axis=1).astype(BF16)
    for n in range(TP):
        rows = pl.ds(pl.multiple_of((own_ref[2] + n) % TP * TOK, TOK), TOK)
        attended = part_ref[rows, :] + dot(qdev_ref[rows, :], carried, NT)
        heads = []
        for h in range(2):
            head = attended[:, h * DV : (h + 1) * DV]
            heads.append(head * lax.rsqrt(jnp.mean(head * head, axis=-1, keepdims=True) + EPS))
        gate = gate_ref[rows, :].astype(F32)
        mixed = jnp.concatenate(heads, axis=1) * gain_ref[...] * (gate * jax.nn.sigmoid(gate))
        out_refs[n][...] = mixed.astype(BF16)


def normalize(x):
    return x * lax.rsqrt(jnp.mean(x * x, axis=-1, keepdims=True) + EPS)


def project_kernel(
    own_ref, slots_ref, mixed_0, mixed_1, mixed_2, mixed_3, weight_ref, stream_ref, mix_ref,
    ffn_ref, residual_ref, normed_ref, sent_ref, acc_ref, rows_ref,
):
    step = pl.program_id(0)

    @pl.when(step == 0)
    def _():
        acc_ref[...] = dot(mixed_0[...], weight_ref[...])
        sent_ref[...] = jnp.zeros_like(sent_ref)

    for n, mixed_ref in enumerate((mixed_1, mixed_2, mixed_3)):

        @pl.when(step == n + 1)
        def _(mixed_ref=mixed_ref):
            acc_ref[...] += dot(mixed_ref[...], weight_ref[...])

    @pl.when(step == TP - 1)
    def _():
        projected = normalize(acc_ref[...]) * mix_ref[...]
        residual = (stream_ref[...].astype(F32) + projected).astype(BF16)
        residual_ref[...] = residual
        normed = (normalize(residual.astype(F32)) * ffn_ref[...]).astype(BF16)
        normed_ref[...] = normed
        wide = normed.astype(F32)
        for j in range(COLS):
            rows_ref[pl.ds(j, TOK, stride=COLS), :] = wide[:, j * LANES : (j + 1) * LANES]

        def place(t, carry):
            line = rows_ref[pl.ds(pl.multiple_of(t * COLS, COLS), COLS), :].astype(BF16)
            for k in range(TOPK):
                sent_ref[slots_ref[k, t]] = line
            return carry

        lax.fori_loop(0, TOK, place, 0, unroll=8)


def pack_shared_kernel(gate_ref, up_ref, down_ref, after_ref, *out_refs):
    half = CHUNKS // 2
    for i in range(CHUNKS):
        rows = pl.ds(i * CHUNK, CHUNK)
        out_ref, at = out_refs[i // half], i % half
        out_ref[at, pl.ds(0, CHUNK), pl.ds(0, LANES)] = gate_ref[rows, :]
        out_ref[at, pl.ds(0, CHUNK), pl.ds(LANES, LANES)] = up_ref[rows, :]
        out_ref[at, pl.ds(CHUNK, LANES), :] = down_ref[:, rows]


def pack_shared(gate, up, down, after):
    return pl.pallas_call(
        pack_shared_kernel,
        out_shape=(shape((CHUNKS // 2, CHUNK + LANES, CHUNK), BF16),) * 2,
        in_specs=[vmem()] * 3 + [anywhere()],
        out_specs=(vmem(),) * 2,
        compiler_params=params(),
        cost_estimate=cost(1_000_000, 3_200_000),
        name="pack_shared",
    )(gate, up, down, after)


def silu(x):
    return x * jax.nn.sigmoid(x)


def expert_copies(gates, ups, downs, gate_ref, up_ref, down_ref, sems):
    copies = []
    for n in range(len(gates)):
        copies.append([
            pltpu.make_async_copy(gates[n], gate_ref.at[n], sems.at[0, n]),
            pltpu.make_async_copy(ups[n], up_ref.at[n], sems.at[1, n]),
        ])
        if len(downs) == len(gates):
            copies[n].append(pltpu.make_async_copy(downs[n], down_ref.at[n], sems.at[2, n]))
        else:
            half = down_ref.shape[1] // 2
            copies[n] += [
                pltpu.make_async_copy(
                    downs[h], down_ref.at[n, pl.ds(h * half, half)], sems.at[2 + h, n]
                )
                for h in range(2)
            ]
    for group in copies:
        for copy in group:
            copy.start()
    return copies


def expert_near_kernel(*refs):
    sent_ref, gates, ups, downs = refs[0], refs[1:4], refs[4:7], refs[7:10]
    rows_ref, acc_ref, sent, lines_ref, gate_ref, up_ref, down_ref, sent_sems, sems = refs[10:]
    part = SLOTS // PIECES
    arrivals = [
        pltpu.make_async_copy(
            sent_ref.at[pl.ds(p * part * COLS, part * COLS)],
            sent.at[pl.ds(p * part * COLS, part * COLS)],
            sent_sems.at[p],
        )
        for p in range(PIECES)
    ]
    for copy in arrivals:
        copy.start()
    copies = expert_copies(gates, ups, downs, gate_ref, up_ref, down_ref, sems)
    for p, copy in enumerate(arrivals):
        copy.wait()
        span = pl.ds(p * part * COLS, part * COLS)
        lines_ref[span, :] = sent[span, :].astype(F32)
        for j in range(COLS):
            rows_ref[pl.ds(p * part, part), j * LANES : (j + 1) * LANES] = lines_ref[
                pl.ds(p * part * COLS + j, part, stride=COLS), :
            ].astype(BF16)
    for n, group in enumerate(copies):
        group[0].wait()
        group[1].wait()
        rows = rows_ref[...]
        hidden = (silu(dot(rows, gate_ref[n])) * dot(rows, up_ref[n])).astype(BF16)
        group[2].wait()
        for j in range(CHUNKS):
            columns = pl.ds(j * CHUNK, CHUNK)
            product = dot(hidden, down_ref[n, :, columns])
            if n == 0:
                acc_ref[:, columns] = product
            else:
                acc_ref[:, columns] += product


def expert_far_kernel(*refs):
    rows_ref, acc_ref, gates, ups, downs, out_ref = refs[0], refs[1], refs[2:3], refs[3:4], refs[4:6], refs[6]
    sent, lines_ref, gate_ref, up_ref, down_ref, sems, out_sems = refs[7:]
    part = SLOTS // PIECES
    group = expert_copies(gates, ups, downs, gate_ref, up_ref, down_ref, sems)[0]
    for copy in group:
        copy.wait()
    outs = []
    for p in range(PIECES):
        block = pl.ds(p * part, part)
        rows = rows_ref[block, :]
        hidden = (silu(dot(rows, gate_ref[0])) * dot(rows, up_ref[0])).astype(BF16)
        for j in range(CHUNKS):
            columns = pl.ds(j * CHUNK, CHUNK)
            total = acc_ref[block, columns] + dot(hidden, down_ref[0, :, columns])
            for i in range(CHUNK // LANES):
                lines_ref[
                    pl.ds(p * part * COLS + j * (CHUNK // LANES) + i, part, stride=COLS), :
                ] = total[:, i * LANES : (i + 1) * LANES]
        span = pl.ds(p * part * COLS, part * COLS)
        sent[span, :] = lines_ref[span, :].astype(BF16)
        copy = pltpu.make_async_copy(sent.at[span], out_ref.at[span], out_sems.at[p])
        copy.start()
        outs.append(copy)
    for copy in outs:
        copy.wait()


def shared_kernel(*refs):
    rows_ref, shards, out_ref, weight_ref, sems = refs[0], refs[1:9], refs[9], refs[10], refs[11]
    half = CHUNKS // 2
    copies = [
        pltpu.make_async_copy(
            shards[2 * n + h], weight_ref.at[n, pl.ds(h * half, half)], sems.at[n, h]
        )
        for n in range(TP)
        for h in range(2)
    ]
    for copy in copies:
        copy.start()
    for n in range(TP):
        copies[2 * n].wait()
        copies[2 * n + 1].wait()
        joint = jnp.zeros((TOK, 2 * LANES), F32)
        for i in range(CHUNKS):
            columns = pl.ds(i * CHUNK, CHUNK)
            joint = joint + dot(rows_ref[:, columns], weight_ref[n, i, 0:CHUNK, :])
        hidden = (silu(joint[:, :LANES]) * joint[:, LANES:]).astype(BF16)
        for i in range(CHUNKS):
            columns = pl.ds(i * CHUNK, CHUNK)
            product = dot(hidden, weight_ref[n, i, CHUNK:, :])
            if n == 0:
                out_ref[:, columns] = product
            else:
                out_ref[:, columns] += product


def combine_kernel(
    slots_ref, weights_ref, back_ref, shared_ref, residual_ref, gain_ref, out_ref, lines_ref, mix_ref
):
    def gather(t, carry):
        line = jnp.zeros((COLS, LANES), F32)
        for k in range(TOPK):
            line = line + back_ref[slots_ref[k, t]].astype(F32) * weights_ref[k, t]
        lines_ref[pl.ds(pl.multiple_of(t * COLS, COLS), COLS), :] = line
        return carry

    lax.fori_loop(0, TOK, gather, 0, unroll=8)
    for j in range(COLS):
        columns = slice(j * LANES, (j + 1) * LANES)
        mix_ref[:, columns] = shared_ref[:, columns] + lines_ref[pl.ds(j, TOK, stride=COLS), :]
    out_ref[...] = (
        residual_ref[...].astype(F32) + normalize(mix_ref[...]) * gain_ref[...]
    ).astype(BF16)


def vmem():
    return pl.BlockSpec(memory_space=pltpu.VMEM)


def anywhere():
    return pl.BlockSpec(memory_space=pltpu.HBM)


def shift(array, hops):
    return lax.ppermute(array, "tp", [(i, (i + hops) % TP) for i in range(TP)])


def smem():
    return pl.BlockSpec(memory_space=pltpu.SMEM)


def params(mib=60, **extra):
    return pltpu.CompilerParams(vmem_limit_bytes=mib * 1024 * 1024, **extra)


def shape(dims, kind):
    return jax.ShapeDtypeStruct(dims, kind)


def cost(flops, moved):
    return pl.CostEstimate(flops=flops, bytes_accessed=moved, transcendentals=0)


def whole(dims):
    return pl.BlockSpec(dims, lambda i, *_: (0,) * len(dims))


def body(
    stream,
    queries,
    key_rows,
    values,
    out_gate,
    fwd_decay,
    bwd_decay,
    head_gain,
    out_proj,
    mix_gain,
    ffn_gain,
    moe_gain,
    routes,
    route_weight,
    expert_gate,
    expert_up,
    expert_down,
    shared_gate,
    shared_up,
    shared_down,
):
    own = jnp.stack([lax.axis_index(axes) for axes in (PLANE, "sp_0", "tp", "sp_2")])
    own = own.astype(jnp.int32)
    gate, up, down = expert_gate[0], expert_up[0], expert_down[0]
    gate_left = shift(gate, 1)
    gate_right = shift(gate, -1)
    up_left = shift(up, 1)
    up_right = shift(up, -1)

    tables = [jnp.asarray(table) for table in rope_tables()]
    msg, keys, cumuls, states = pl.pallas_call(
        states_kernel,
        out_shape=(
            shape((XC, MSG, LANES), BF16),
            shape((SPAN, LANES), F32),
            shape((2, SPAN, LANES), F32),
            shape((2, SPAN // BLK, DV, LANES), F32),
        ),
        in_specs=[smem()] + [vmem()] * 7,
        out_specs=(vmem(),) * 4,
        compiler_params=params(),
        cost_estimate=cost(200_000_000, 4_000_000),
        name="states",
    )(own, key_rows, values, fwd_decay, bwd_decay, *tables)
    in_plane = lax.all_to_all(msg, PLANE, split_axis=0, concat_axis=0, tiled=True)
    part, qdev, flat_slots = pl.pallas_call(
        attention_kernel,
        out_shape=(
            shape((SPAN, 2 * DV), F32),
            shape((SPAN, 2 * LANES), BF16),
            shape((TOPK, TOK), jnp.int32),
        ),
        in_specs=[smem()] + [vmem()] * 9,
        out_specs=(vmem(),) * 3,
        compiler_params=params(),
        cost_estimate=cost(400_000_000, 4_000_000),
        name="attention",
    )(own, queries, values, keys, cumuls, states, *tables, routes.T)
    inner, logs, msg = pl.pallas_call(
        plane_kernel,
        out_shape=(
            shape((2, DV, LANES), F32),
            shape((8, LANES), F32),
            shape((Z, HALF_MSG, LANES), BF16),
        ),
        in_specs=[smem(), vmem()],
        out_specs=(vmem(),) * 3,
        compiler_params=params(40),
        cost_estimate=cost(10_000_000, 1_000_000),
        name="plane",
    )(own, in_plane)
    planes = lax.all_to_all(msg, "sp_0", split_axis=0, concat_axis=0, tiled=True)
    mixed = pl.pallas_call(
        readout_kernel,
        out_shape=(shape((TOK, 2 * DV), BF16),) * TP,
        in_specs=[smem()] + [vmem()] * 7,
        out_specs=(vmem(),) * TP,
        compiler_params=params(60),
        cost_estimate=cost(100_000_000, 3_000_000),
        name="readout",
    )(
        own, planes, inner, logs, part, qdev, out_gate, head_gain.reshape(1, -1),
    )
    mixed = [shift(piece, n) if n else piece for n, piece in enumerate(mixed)]

    down_left = shift(down, 1)
    down_right = shift(down, -1)
    gate_far = shift(gate_left, 1)
    up_far = shift(up_right, -1)
    down_far_1 = shift(down_left[: down.shape[0] // 2], 1)
    down_far_2 = shift(down_right[down.shape[0] // 2 :], -1)

    residual, normed, sent = pl.pallas_call(
        project_kernel,
        out_shape=(
            shape((TOK, D), BF16),
            shape((TOK, D), BF16),
            shape((SLOTS, COLS, LANES), BF16),
        ),
        grid_spec=pltpu.PrefetchScalarGridSpec(
            num_scalar_prefetch=2,
            grid=(TP,),
            in_specs=[whole((TOK, 2 * DV))] * TP
            + [
                pl.BlockSpec((2 * DV, D), lambda i, own, _: ((own[2] + TP - i) % TP, 0)),
                whole((TOK, D)),
                whole((1, D)),
                whole((1, D)),
            ],
            out_specs=(whole((TOK, D)), whole((TOK, D)), whole((SLOTS, COLS, LANES))),
            scratch_shapes=[pltpu.VMEM((TOK, D), F32), pltpu.VMEM((TOK * COLS, LANES), F32)],
        ),
        compiler_params=params(59, dimension_semantics=("arbitrary",)),
        cost_estimate=cost(600_000_000, 8_000_000),
        name="project",
    )(own, flat_slots, *mixed, out_proj, stream, mix_gain.reshape(1, -1), ffn_gain.reshape(1, -1))

    arrived = lax.all_to_all(
        sent.reshape(EXPERTS, CAP * COLS, LANES), SP, split_axis=0, concat_axis=0, tiled=True
    )
    width = gate.shape[1]
    near = TP - 1
    rows, partial = pl.pallas_call(
        expert_near_kernel,
        out_shape=(shape((SLOTS, D), BF16), shape((SLOTS, D), F32)),
        in_specs=[anywhere()] * (1 + 3 * near),
        out_specs=(vmem(), vmem()),
        scratch_shapes=[
            pltpu.VMEM((SLOTS * COLS, LANES), BF16),
            pltpu.VMEM((SLOTS * COLS, LANES), F32),
            pltpu.VMEM((near, D, width), BF16),
            pltpu.VMEM((near, D, width), BF16),
            pltpu.VMEM((near, width, D), BF16),
            pltpu.SemaphoreType.DMA((PIECES,)),
            pltpu.SemaphoreType.DMA((3, near)),
        ],
        compiler_params=params(26),
        cost_estimate=cost(3_600_000_000, 16_000_000),
        name="experts_near",
    )(
        arrived.reshape(SLOTS * COLS, LANES),
        gate, gate_left, gate_right, up, up_left, up_right, down, down_left, down_right,
    )
    done = pl.pallas_call(
        expert_far_kernel,
        out_shape=shape((SLOTS * COLS, LANES), BF16),
        in_specs=[vmem(), vmem()] + [anywhere()] * 4,
        out_specs=anywhere(),
        scratch_shapes=[
            pltpu.VMEM((SLOTS * COLS, LANES), BF16),
            pltpu.VMEM((SLOTS * COLS, LANES), F32),
            pltpu.VMEM((1, D, width), BF16),
            pltpu.VMEM((1, D, width), BF16),
            pltpu.VMEM((1, width, D), BF16),
            pltpu.SemaphoreType.DMA((4, 1)),
            pltpu.SemaphoreType.DMA((PIECES,)),
        ],
        compiler_params=params(20),
        cost_estimate=cost(1_200_000_000, 8_000_000),
        name="experts_far",
    )(rows, partial, gate_far, up_far, down_far_1, down_far_2)
    back = lax.all_to_all(
        done.reshape(EXPERTS, CAP * COLS, LANES), SP, split_axis=0, concat_axis=0, tiled=True
    )
    packed = pack_shared(shared_gate, shared_up, shared_down, residual)
    shared_left, shared_right = [None, None], [None, None]
    for h in range(2):
        shared_left[h] = shift(packed[h], 1)
        shared_right[h] = shift(packed[h], -1)
    shared_far_0 = shift(shared_left[0], 1)
    shared_far_1 = shift(shared_right[1], -1)
    shared = pl.pallas_call(
        shared_kernel,
        out_shape=shape((TOK, D), F32),
        in_specs=[vmem()] + [anywhere()] * 8,
        out_specs=vmem(),
        scratch_shapes=[
            pltpu.VMEM((TP, CHUNKS, CHUNK + LANES, CHUNK), BF16),
            pltpu.SemaphoreType.DMA((TP, 2)),
        ],
        compiler_params=params(60),
        cost_estimate=cost(800_000_000, 8_000_000),
        name="shared",
    )(normed, *packed, *shared_left, *shared_right, shared_far_0, shared_far_1)
    return pl.pallas_call(
        combine_kernel,
        out_shape=shape((TOK, D), BF16),
        in_specs=[smem(), smem()] + [vmem()] * 4,
        out_specs=vmem(),
        scratch_shapes=[pltpu.VMEM((TOK * COLS, LANES), F32), pltpu.VMEM((TOK, D), F32)],
        compiler_params=params(40),
        cost_estimate=cost(5_000_000, 4_000_000),
        name="combine",
    )(
        flat_slots, route_weight.T, back.reshape(SLOTS, COLS, LANES),
        shared, residual, moe_gain.reshape(1, -1),
    )


def solution(mesh):
    finer = Mesh(mesh.devices.reshape(8, 4, 2, mesh.shape["tp"]), ("sp_0", "sp_1", "sp_2", "tp"))
    placed = (
        P(SP_TP, None),
        P(SP, "tp"),
        P(SP, "tp"),
        P(SP, "tp"),
        P(SP, "tp"),
        P(SP, "tp"),
        P(SP, "tp"),
        P("tp"),
        P(),
        P(),
        P(),
        P(),
        P(SP_TP, None),
        P(SP_TP, None),
        P(SP, None, "tp"),
        P(SP, None, "tp"),
        P(SP, "tp", None),
        P(None, "tp"),
        P(None, "tp"),
        P("tp", None),
    )

    return jax.shard_map(
        body, mesh=finer, in_specs=placed, out_specs=P(SP_TP, None), check_vma=False
    )
```

```python
import jax
import jax.numpy as jnp
import numpy as np
from jax import lax
from jax.experimental import pallas as pl
from jax.experimental.pallas import tpu as pltpu
from jax.sharding import Mesh
from jax.sharding import PartitionSpec as P


KEY_CHANNELS = 64
DV = 128
BLK = 128
TOPK = 2
CAP = 6
Z, XC, TP = 8, 8, 4
SP = ("sp_0", "sp_1", "sp_2")
PLANE = ("sp_1", "sp_2")
SP_TP = ("sp_0", "sp_1", "sp_2", "tp")
SPAN = 512
TOK = 128
D = 2048
EXPERTS = 64
SLOTS = EXPERTS * CAP
LANES = 128
COLS = D // LANES
CHUNK = 256
PIECES = 4
FAR_PIECES = 2
CHUNKS = D // CHUNK
MSG = 272
HALF_MSG = 144

EPS = 1e-06
GATE_NORM = 16.0
ROPE_BASE = 10000.0
F32 = jnp.float32
BF16 = jnp.bfloat16
NT = (((1,), (1,)), ((), ()))
TN = (((0,), (0,)), ((), ()))


def rope_tables():
    half = KEY_CHANNELS // 2
    frequency = ROPE_BASE ** (-np.arange(half, dtype=np.float64) / half)
    lanes = np.tile(frequency, LANES // half)
    tables = []
    for count, step in ((BLK, 1), (SPAN // BLK, BLK), (Z * XC, SPAN)):
        angles = (np.arange(count) * step)[:, None] * lanes[None, :]
        tables.append(np.stack([np.cos(angles), np.sin(angles)], axis=0).astype(np.float32))
    return tables[0], tables[1].reshape(-1, LANES), tables[2].swapaxes(0, 1)


def dot(a, b, dims=(((1,), (0,)), ((), ()))):
    return lax.dot_general(a, b, dims, preferred_element_type=F32)


def iota(shape, axis):
    return lax.broadcasted_iota(jnp.int32, shape, axis)


def log_sigmoid(x):
    return jnp.minimum(x, 0.0) - jnp.log1p(jnp.exp(-jnp.abs(x)))


def spread(state, low):
    return jnp.concatenate([jnp.where(low, state, 0.0), jnp.where(low, 0.0, state)], axis=0)


def split_rows(rows):
    pieces = []
    for row in rows:
        high = row.astype(BF16)
        pieces += [high.astype(F32), row - high.astype(F32)]
    row_id = iota((16, LANES), 0)
    out = jnp.zeros((16, LANES), F32)
    for i, piece in enumerate(pieces):
        out = jnp.where(row_id == i, piece, out)
    return out


class Block:
    def __init__(self, own_ref, local_ref, block_ref, base_ref):
        self.count = SPAN // BLK
        lane = iota((BLK, LANES), 1)
        self.low = lane < KEY_CHANNELS
        self.front = lane % KEY_CHANNELS < KEY_CHANNELS // 2
        self.row, self.col = iota((BLK, BLK), 0), iota((BLK, BLK), 1)
        self.local, self.blocks = local_ref, block_ref
        self.base = base_ref[own_ref[1] * XC + own_ref[0]]

    def tables(self, n):
        def add(a, b):
            return a[0] * b[0] - a[1] * b[1], a[1] * b[0] + a[0] * b[1]

        span = self.base[0:1, :], self.base[1:2, :]
        m = self.count + n
        start = add(span, (self.blocks[n : n + 1, :], self.blocks[m : m + 1, :]))
        cosine, sine = add(start, (self.local[0], self.local[1]))
        return cosine, jnp.where(self.front, -sine, sine)

    def rotate(self, u, tables):
        swapped = jnp.where(
            self.front,
            pltpu.roll(u, LANES - KEY_CHANNELS // 2, 1),
            pltpu.roll(u, KEY_CHANNELS // 2, 1),
        )
        return u * tables[0] + swapped * tables[1]

    def decays(self, log_ref, forward):
        tri = (self.row >= self.col if forward else self.row <= self.col).astype(BF16)
        parts = []
        for n in range(self.count):
            log = log_sigmoid(log_ref[pl.ds(n * BLK, BLK), :]) * (1.0 / GATE_NORM)
            for _ in range(3):
                part = log.astype(BF16)
                parts.append(part)
                log = log - part.astype(F32)
        sums = dot(tri, jnp.concatenate(parts, axis=1))
        pieces = [sums[:, i * LANES : (i + 1) * LANES] for i in range(3 * self.count)]
        return [sum(pieces[3 * n + 1 : 3 * n + 3], pieces[3 * n]) for n in range(self.count)]


def states_kernel(
    own_ref, k_ref, v_ref, fd_ref, bd_ref, local_ref, block_ref, base_ref,
    msg_ref, key_ref, cumul_ref, states_ref,
):
    block = Block(own_ref, local_ref, block_ref, base_ref)
    count, low = block.count, block.low
    updates, lasts = ([], []), ([], [])
    decays = [block.decays(fd_ref, True), block.decays(bd_ref, False)]
    for n in range(count):
        rows = pl.ds(n * BLK, BLK)
        k = block.rotate(k_ref[rows, :].astype(F32), block.tables(n))
        key_ref[rows, :] = k
        v = v_ref[rows, :]
        for d in range(2):
            cumul = decays[d][n]
            end = BLK - 1 if d == 0 else 0
            total = cumul[end : end + 1, :]
            cumul_ref[d, rows, :] = cumul
            k_out = k * jnp.exp(total - cumul)
            product = dot(v, k_out.astype(BF16), TN)
            updates[d].append(jnp.where(low, product[:DV], product[DV:]))
            lasts[d].append(total)
    finals, sums = [], []
    for d in range(2):
        state, logs = jnp.zeros((DV, LANES), F32), jnp.zeros((1, LANES), F32)
        for n in range(count) if d == 0 else reversed(range(count)):
            states_ref[d, n] = state
            state = state * jnp.exp(lasts[d][n]) + updates[d][n]
            logs = logs + lasts[d][n]
        finals.append(state.astype(BF16))
        sums.append(logs)
    tail = split_rows(sums).astype(BF16)
    for j in range(XC):
        msg_ref[j, pl.ds(0, DV), :] = finals[0]
        msg_ref[j, pl.ds(DV, DV), :] = finals[1]
        msg_ref[j, pl.ds(2 * DV, 16), :] = tail


def attention_kernel(
    own_ref, q_ref, v_ref, key_ref, cumul_ref, states_ref, local_ref, block_ref, base_ref,
    routes_ref,
    part_ref, qdev_ref, slots_ref,
):
    block = Block(own_ref, local_ref, block_ref, base_ref)
    count, low, row, col = block.count, block.low, block.row, block.col
    row2, col2 = iota((BLK, 2 * BLK), 0), iota((BLK, 2 * BLK), 1) % BLK
    wide_low = iota((BLK, 2 * DV), 1) < DV
    zero_row = jnp.zeros((1, LANES), F32)
    lasts = [
        [cumul_ref[0, pl.ds(n * BLK + BLK - 1, 1), :] for n in range(count)],
        [cumul_ref[1, pl.ds(n * BLK, 1), :] for n in range(count)],
    ]
    for n in range(count):
        rows = pl.ds(n * BLK, BLK)
        scale = KEY_CHANNELS ** (-0.5)
        q = block.rotate(q_ref[rows, :].astype(F32) * scale, block.tables(n))
        k = key_ref[rows, :]
        v = v_ref[rows, :].astype(F32)
        v_bd = jnp.concatenate(
            [jnp.where(wide_low, v, 0.0), jnp.where(wide_low, 0.0, v)], axis=0
        ).astype(BF16)
        scores = jnp.zeros((BLK, 2 * BLK), F32)
        q_ins, carried, reaches = [], [], []
        for d in range(2):
            cumul = cumul_ref[d, rows, :]
            at = BLK // 2 - 1 if d == 0 else BLK // 2
            middle = cumul[at : at + 1, :]
            offset = cumul - middle
            q_scaled = q * jnp.exp(offset)
            k_scaled = k * jnp.exp(-offset)
            both = dot(q_scaled.astype(BF16), spread(k_scaled, low).astype(BF16), NT)
            reach = row2 >= col2 if d == 0 else row2 <= col2
            scores = scores + jnp.where(reach, both, 0.0)
            q_ins.append(q_scaled * jnp.exp(middle))
            carried.append(spread(states_ref[d, n], low))
            passed = range(n) if d == 0 else range(n + 1, count)
            reaches.append(sum((lasts[d][m] for m in passed), zero_row))
        q_in = jnp.concatenate(q_ins, axis=1)
        within = dot(scores.astype(BF16), v_bd)
        across = dot(q_in.astype(BF16), jnp.concatenate(carried, axis=1).astype(BF16), NT)
        part_ref[rows, :] = within + across
        qdev_ref[rows, :] = (q_in * jnp.exp(jnp.concatenate(reaches, axis=1))).astype(BF16)

    expert = iota((EXPERTS, TOK), 0)
    picks = [routes_ref[k : k + 1, :] == expert for k in range(TOPK)]
    chosen = jnp.zeros((EXPERTS, TOK), F32)
    for pick in picks:
        chosen = chosen + pick.astype(F32)
    strict = (row < col).astype(BF16)
    before = dot(chosen.astype(BF16), strict)
    place = before + (CAP * expert).astype(F32)
    for k, pick in enumerate(picks):
        found = jnp.sum(jnp.where(pick, place, 0.0), axis=0, keepdims=True)
        slots_ref[k : k + 1, :] = found.astype(jnp.int32)


def compose_gathered(own, gathered_ref, length, shared_place=False):
    results = []
    for forward in (True, False):
        start, tail_at, first = (0, 2 * DV, 0) if forward else (DV, 2 * DV, 2)
        if shared_place:
            start, tail_at, first = 0, DV, 0
        state, logs = jnp.zeros((DV, LANES), F32), jnp.zeros((1, LANES), F32)
        inner, inner_logs = state, logs
        for step in range(length):
            k = step if forward else length - 1 - step
            here = own == k
            inner = jnp.where(here, state, inner)
            inner_logs = jnp.where(here, logs, inner_logs)
            tail = gathered_ref[k, pl.ds(tail_at, 16), :].astype(F32)
            log = tail[first : first + 1, :] + tail[first + 1 : first + 2, :]
            state = state * jnp.exp(log) + gathered_ref[k, pl.ds(start, DV), :].astype(F32)
            logs = logs + log
        results.append((state, logs, inner, inner_logs))
    return results


def plane_kernel(own_ref, gathered_ref, inner_ref, logs_ref, msg_ref):
    forward, backward = compose_gathered(own_ref[0], gathered_ref, XC)
    inner_ref[0] = forward[2]
    inner_ref[1] = backward[2]
    row_id = iota((8, LANES), 0)
    logs_ref[...] = jnp.where(row_id == 0, forward[3], jnp.where(row_id == 1, backward[3], 0.0))
    for j in range(Z):
        later = own_ref[1] < j
        msg_ref[j, pl.ds(0, DV), :] = jnp.where(later, forward[0], backward[0]).astype(BF16)
        logs = jnp.where(later, forward[1], backward[1])
        msg_ref[j, pl.ds(DV, 16), :] = split_rows([logs]).astype(BF16)


def readout_kernel(
    own_ref, gathered_ref, inner_ref, logs_ref, part_ref, qdev_ref, gate_ref, gain_ref, *out_refs
):
    forward, backward = compose_gathered(own_ref[1], gathered_ref, Z, shared_place=True)
    low = iota((DV, LANES), 1) < KEY_CHANNELS
    carry_f = inner_ref[0] + forward[2] * jnp.exp(logs_ref[0:1, :])
    carry_b = inner_ref[1] + backward[2] * jnp.exp(logs_ref[1:2, :])
    carried = jnp.concatenate([spread(carry_f, low), spread(carry_b, low)], axis=1).astype(BF16)
    for n in range(TP):
        rows = pl.ds(pl.multiple_of((own_ref[2] + n) % TP * TOK, TOK), TOK)
        attended = part_ref[rows, :] + dot(qdev_ref[rows, :], carried, NT)
        heads = []
        for h in range(2):
            head = attended[:, h * DV : (h + 1) * DV]
            heads.append(head * lax.rsqrt(jnp.mean(head * head, axis=-1, keepdims=True) + EPS))
        gate = gate_ref[rows, :].astype(F32)
        mixed = jnp.concatenate(heads, axis=1) * gain_ref[...] * (gate * jax.nn.sigmoid(gate))
        out_refs[n][...] = mixed.astype(BF16)


def normalize(x):
    return x * lax.rsqrt(jnp.mean(x * x, axis=-1, keepdims=True) + EPS)


def project_kernel(
    own_ref, slots_ref, mixed_0, mixed_1, mixed_2, mixed_3, weight_ref, stream_ref, mix_ref,
    ffn_ref, residual_ref, normed_ref, sent_ref, acc_ref, rows_ref,
):
    step = pl.program_id(0)

    @pl.when(step == 0)
    def _():
        acc_ref[...] = dot(mixed_0[...], weight_ref[...])
        sent_ref[...] = jnp.zeros_like(sent_ref)

    for n, mixed_ref in enumerate((mixed_1, mixed_2, mixed_3)):

        @pl.when(step == n + 1)
        def _(mixed_ref=mixed_ref):
            acc_ref[...] += dot(mixed_ref[...], weight_ref[...])

    @pl.when(step == TP - 1)
    def _():
        projected = normalize(acc_ref[...]) * mix_ref[...]
        residual = (stream_ref[...].astype(F32) + projected).astype(BF16)
        residual_ref[...] = residual
        normed = (normalize(residual.astype(F32)) * ffn_ref[...]).astype(BF16)
        normed_ref[...] = normed
        wide = normed.astype(F32)
        for j in range(COLS):
            rows_ref[pl.ds(j, TOK, stride=COLS), :] = wide[:, j * LANES : (j + 1) * LANES]

        def place(t, carry):
            line = rows_ref[pl.ds(pl.multiple_of(t * COLS, COLS), COLS), :].astype(BF16)
            for k in range(TOPK):
                sent_ref[slots_ref[k, t]] = line
            return carry

        lax.fori_loop(0, TOK, place, 0, unroll=8)


def pack_shared_kernel(gate_ref, up_ref, down_ref, after_ref, *out_refs):
    half = CHUNKS // 2
    for i in range(CHUNKS):
        rows = pl.ds(i * CHUNK, CHUNK)
        out_ref, at = out_refs[i // half], i % half
        out_ref[at, pl.ds(0, CHUNK), pl.ds(0, LANES)] = gate_ref[rows, :]
        out_ref[at, pl.ds(0, CHUNK), pl.ds(LANES, LANES)] = up_ref[rows, :]
        out_ref[at, pl.ds(CHUNK, LANES), :] = down_ref[:, rows]


def pack_shared(gate, up, down, after):
    return pl.pallas_call(
        pack_shared_kernel,
        out_shape=(shape((CHUNKS // 2, CHUNK + LANES, CHUNK), BF16),) * 2,
        in_specs=[vmem()] * 3 + [anywhere()],
        out_specs=(vmem(),) * 2,
        compiler_params=params(),
        cost_estimate=cost(1_000_000, 3_200_000),
        name="pack_shared",
    )(gate, up, down, after)


def silu(x):
    return x * jax.nn.sigmoid(x)


def expert_copies(gates, ups, downs, gate_ref, up_ref, down_ref, sems):
    copies = []
    for n in range(len(gates)):
        copies.append([
            pltpu.make_async_copy(gates[n], gate_ref.at[n], sems.at[0, n]),
            pltpu.make_async_copy(ups[n], up_ref.at[n], sems.at[1, n]),
        ])
        if len(downs) == len(gates):
            copies[n].append(pltpu.make_async_copy(downs[n], down_ref.at[n], sems.at[2, n]))
        else:
            half = down_ref.shape[1] // 2
            copies[n] += [
                pltpu.make_async_copy(
                    downs[h], down_ref.at[n, pl.ds(h * half, half)], sems.at[2 + h, n]
                )
                for h in range(2)
            ]
    for group in copies:
        for copy in group:
            copy.start()
    return copies


def expert_near_kernel(*refs):
    sent_ref, gates, ups, downs = refs[0], refs[1:4], refs[4:7], refs[7:10]
    rows_ref, acc_ref, sent, lines_ref, gate_ref, up_ref, down_ref, sent_sems, sems = refs[10:]
    part = SLOTS // PIECES
    arrivals = [
        pltpu.make_async_copy(
            sent_ref.at[pl.ds(p * part * COLS, part * COLS)],
            sent.at[pl.ds(p * part * COLS, part * COLS)],
            sent_sems.at[p],
        )
        for p in range(PIECES)
    ]
    for copy in arrivals:
        copy.start()
    copies = expert_copies(gates, ups, downs, gate_ref, up_ref, down_ref, sems)
    for p, copy in enumerate(arrivals):
        copy.wait()
        span = pl.ds(p * part * COLS, part * COLS)
        lines_ref[span, :] = sent[span, :].astype(F32)
        for j in range(COLS):
            rows_ref[pl.ds(p * part, part), j * LANES : (j + 1) * LANES] = lines_ref[
                pl.ds(p * part * COLS + j, part, stride=COLS), :
            ].astype(BF16)
    for n, group in enumerate(copies):
        group[0].wait()
        group[1].wait()
        rows = rows_ref[...]
        hidden = (silu(dot(rows, gate_ref[n])) * dot(rows, up_ref[n])).astype(BF16)
        group[2].wait()
        for j in range(CHUNKS):
            columns = pl.ds(j * CHUNK, CHUNK)
            product = dot(hidden, down_ref[n, :, columns])
            if n == 0:
                acc_ref[:, columns] = product
            else:
                acc_ref[:, columns] += product


def expert_far_kernel(*refs):
    rows_ref, acc_ref, gates, ups, downs, out_ref = refs[0], refs[1], refs[2:3], refs[3:4], refs[4:6], refs[6]
    sent, lines_ref, gate_ref, up_ref, down_ref, sems, out_sems = refs[7:]
    part = SLOTS // FAR_PIECES
    group = expert_copies(gates, ups, downs, gate_ref, up_ref, down_ref, sems)[0]
    for copy in group:
        copy.wait()
    outs = []
    for p in range(FAR_PIECES):
        block = pl.ds(p * part, part)
        rows = rows_ref[block, :]
        hidden = (silu(dot(rows, gate_ref[0])) * dot(rows, up_ref[0])).astype(BF16)
        for j in range(CHUNKS):
            columns = pl.ds(j * CHUNK, CHUNK)
            total = acc_ref[block, columns] + dot(hidden, down_ref[0, :, columns])
            for i in range(CHUNK // LANES):
                lines_ref[
                    pl.ds(p * part * COLS + j * (CHUNK // LANES) + i, part, stride=COLS), :
                ] = total[:, i * LANES : (i + 1) * LANES]
        span = pl.ds(p * part * COLS, part * COLS)
        sent[span, :] = lines_ref[span, :].astype(BF16)
        copy = pltpu.make_async_copy(sent.at[span], out_ref.at[span], out_sems.at[p])
        copy.start()
        outs.append(copy)
    for copy in outs:
        copy.wait()


def shared_kernel(*refs):
    rows_ref, shards, out_ref, weight_ref, sems = refs[0], refs[1:9], refs[9], refs[10], refs[11]
    half = CHUNKS // 2
    copies = [
        pltpu.make_async_copy(
            shards[2 * n + h], weight_ref.at[n, pl.ds(h * half, half)], sems.at[n, h]
        )
        for n in range(TP)
        for h in range(2)
    ]
    for copy in copies:
        copy.start()
    for n in range(TP):
        copies[2 * n].wait()
        copies[2 * n + 1].wait()
        joint = jnp.zeros((TOK, 2 * LANES), F32)
        for i in range(CHUNKS):
            columns = pl.ds(i * CHUNK, CHUNK)
            joint = joint + dot(rows_ref[:, columns], weight_ref[n, i, 0:CHUNK, :])
        hidden = (silu(joint[:, :LANES]) * joint[:, LANES:]).astype(BF16)
        for i in range(CHUNKS):
            columns = pl.ds(i * CHUNK, CHUNK)
            product = dot(hidden, weight_ref[n, i, CHUNK:, :])
            if n == 0:
                out_ref[:, columns] = product
            else:
                out_ref[:, columns] += product


def combine_kernel(
    slots_ref, weights_ref, back_ref, shared_ref, residual_ref, gain_ref, out_ref, lines_ref, mix_ref
):
    def gather(t, carry):
        line = jnp.zeros((COLS, LANES), F32)
        for k in range(TOPK):
            line = line + back_ref[slots_ref[k, t]].astype(F32) * weights_ref[k, t]
        lines_ref[pl.ds(pl.multiple_of(t * COLS, COLS), COLS), :] = line
        return carry

    lax.fori_loop(0, TOK, gather, 0, unroll=8)
    for j in range(COLS):
        columns = slice(j * LANES, (j + 1) * LANES)
        mix_ref[:, columns] = shared_ref[:, columns] + lines_ref[pl.ds(j, TOK, stride=COLS), :]
    out_ref[...] = (
        residual_ref[...].astype(F32) + normalize(mix_ref[...]) * gain_ref[...]
    ).astype(BF16)


def vmem():
    return pl.BlockSpec(memory_space=pltpu.VMEM)


def anywhere():
    return pl.BlockSpec(memory_space=pltpu.HBM)


def shift(array, hops):
    return lax.ppermute(array, "tp", [(i, (i + hops) % TP) for i in range(TP)])


def smem():
    return pl.BlockSpec(memory_space=pltpu.SMEM)


def params(mib=60, **extra):
    return pltpu.CompilerParams(vmem_limit_bytes=mib * 1024 * 1024, **extra)


def shape(dims, kind):
    return jax.ShapeDtypeStruct(dims, kind)


def cost(flops, moved):
    return pl.CostEstimate(flops=flops, bytes_accessed=moved, transcendentals=0)


def whole(dims):
    return pl.BlockSpec(dims, lambda i, *_: (0,) * len(dims))


def body(
    stream,
    queries,
    key_rows,
    values,
    out_gate,
    fwd_decay,
    bwd_decay,
    head_gain,
    out_proj,
    mix_gain,
    ffn_gain,
    moe_gain,
    routes,
    route_weight,
    expert_gate,
    expert_up,
    expert_down,
    shared_gate,
    shared_up,
    shared_down,
):
    own = jnp.stack([lax.axis_index(axes) for axes in (PLANE, "sp_0", "tp", "sp_2")])
    own = own.astype(jnp.int32)
    gate, up, down = expert_gate[0], expert_up[0], expert_down[0]
    gate_left = shift(gate, 1)
    gate_right = shift(gate, -1)
    up_left = shift(up, 1)
    up_right = shift(up, -1)

    tables = [jnp.asarray(table) for table in rope_tables()]
    msg, keys, cumuls, states = pl.pallas_call(
        states_kernel,
        out_shape=(
            shape((XC, MSG, LANES), BF16),
            shape((SPAN, LANES), F32),
            shape((2, SPAN, LANES), F32),
            shape((2, SPAN // BLK, DV, LANES), F32),
        ),
        in_specs=[smem()] + [vmem()] * 7,
        out_specs=(vmem(),) * 4,
        compiler_params=params(),
        cost_estimate=cost(200_000_000, 4_000_000),
        name="states",
    )(own, key_rows, values, fwd_decay, bwd_decay, *tables)
    in_plane = lax.all_to_all(msg, PLANE, split_axis=0, concat_axis=0, tiled=True)
    part, qdev, flat_slots = pl.pallas_call(
        attention_kernel,
        out_shape=(
            shape((SPAN, 2 * DV), F32),
            shape((SPAN, 2 * LANES), BF16),
            shape((TOPK, TOK), jnp.int32),
        ),
        in_specs=[smem()] + [vmem()] * 9,
        out_specs=(vmem(),) * 3,
        compiler_params=params(),
        cost_estimate=cost(400_000_000, 4_000_000),
        name="attention",
    )(own, queries, values, keys, cumuls, states, *tables, routes.T)
    inner, logs, msg = pl.pallas_call(
        plane_kernel,
        out_shape=(
            shape((2, DV, LANES), F32),
            shape((8, LANES), F32),
            shape((Z, HALF_MSG, LANES), BF16),
        ),
        in_specs=[smem(), vmem()],
        out_specs=(vmem(),) * 3,
        compiler_params=params(40),
        cost_estimate=cost(10_000_000, 1_000_000),
        name="plane",
    )(own, in_plane)
    planes = lax.all_to_all(msg, "sp_0", split_axis=0, concat_axis=0, tiled=True)
    mixed = pl.pallas_call(
        readout_kernel,
        out_shape=(shape((TOK, 2 * DV), BF16),) * TP,
        in_specs=[smem()] + [vmem()] * 7,
        out_specs=(vmem(),) * TP,
        compiler_params=params(60),
        cost_estimate=cost(100_000_000, 3_000_000),
        name="readout",
    )(
        own, planes, inner, logs, part, qdev, out_gate, head_gain.reshape(1, -1),
    )
    mixed = [shift(piece, n) if n else piece for n, piece in enumerate(mixed)]

    down_left = shift(down, 1)
    down_right = shift(down, -1)
    gate_far = shift(gate_left, 1)
    up_far = shift(up_right, -1)
    down_far_1 = shift(down_left[: down.shape[0] // 2], 1)
    down_far_2 = shift(down_right[down.shape[0] // 2 :], -1)

    residual, normed, sent = pl.pallas_call(
        project_kernel,
        out_shape=(
            shape((TOK, D), BF16),
            shape((TOK, D), BF16),
            shape((SLOTS, COLS, LANES), BF16),
        ),
        grid_spec=pltpu.PrefetchScalarGridSpec(
            num_scalar_prefetch=2,
            grid=(TP,),
            in_specs=[whole((TOK, 2 * DV))] * TP
            + [
                pl.BlockSpec((2 * DV, D), lambda i, own, _: ((own[2] + TP - i) % TP, 0)),
                whole((TOK, D)),
                whole((1, D)),
                whole((1, D)),
            ],
            out_specs=(whole((TOK, D)), whole((TOK, D)), whole((SLOTS, COLS, LANES))),
            scratch_shapes=[pltpu.VMEM((TOK, D), F32), pltpu.VMEM((TOK * COLS, LANES), F32)],
        ),
        compiler_params=params(59, dimension_semantics=("arbitrary",)),
        cost_estimate=cost(600_000_000, 8_000_000),
        name="project",
    )(own, flat_slots, *mixed, out_proj, stream, mix_gain.reshape(1, -1), ffn_gain.reshape(1, -1))

    arrived = lax.all_to_all(
        sent.reshape(EXPERTS, CAP * COLS, LANES), SP, split_axis=0, concat_axis=0, tiled=True
    )
    width = gate.shape[1]
    near = TP - 1
    rows, partial = pl.pallas_call(
        expert_near_kernel,
        out_shape=(shape((SLOTS, D), BF16), shape((SLOTS, D), F32)),
        in_specs=[anywhere()] * (1 + 3 * near),
        out_specs=(vmem(), vmem()),
        scratch_shapes=[
            pltpu.VMEM((SLOTS * COLS, LANES), BF16),
            pltpu.VMEM((SLOTS * COLS, LANES), F32),
            pltpu.VMEM((near, D, width), BF16),
            pltpu.VMEM((near, D, width), BF16),
            pltpu.VMEM((near, width, D), BF16),
            pltpu.SemaphoreType.DMA((PIECES,)),
            pltpu.SemaphoreType.DMA((3, near)),
        ],
        compiler_params=params(26),
        cost_estimate=cost(3_600_000_000, 16_000_000),
        name="experts_near",
    )(
        arrived.reshape(SLOTS * COLS, LANES),
        gate, gate_left, gate_right, up, up_left, up_right, down, down_left, down_right,
    )
    done = pl.pallas_call(
        expert_far_kernel,
        out_shape=shape((SLOTS * COLS, LANES), BF16),
        in_specs=[vmem(), vmem()] + [anywhere()] * 4,
        out_specs=anywhere(),
        scratch_shapes=[
            pltpu.VMEM((SLOTS * COLS, LANES), BF16),
            pltpu.VMEM((SLOTS * COLS, LANES), F32),
            pltpu.VMEM((1, D, width), BF16),
            pltpu.VMEM((1, D, width), BF16),
            pltpu.VMEM((1, width, D), BF16),
            pltpu.SemaphoreType.DMA((4, 1)),
            pltpu.SemaphoreType.DMA((FAR_PIECES,)),
        ],
        compiler_params=params(20),
        cost_estimate=cost(1_200_000_000, 8_000_000),
        name="experts_far",
    )(rows, partial, gate_far, up_far, down_far_1, down_far_2)
    back = lax.all_to_all(
        done.reshape(EXPERTS, CAP * COLS, LANES), SP, split_axis=0, concat_axis=0, tiled=True
    )
    packed = pack_shared(shared_gate, shared_up, shared_down, residual)
    shared_left, shared_right = [None, None], [None, None]
    for h in range(2):
        shared_left[h] = shift(packed[h], 1)
        shared_right[h] = shift(packed[h], -1)
    shared_far_0 = shift(shared_left[0], 1)
    shared_far_1 = shift(shared_right[1], -1)
    shared = pl.pallas_call(
        shared_kernel,
        out_shape=shape((TOK, D), F32),
        in_specs=[vmem()] + [anywhere()] * 8,
        out_specs=vmem(),
        scratch_shapes=[
            pltpu.VMEM((TP, CHUNKS, CHUNK + LANES, CHUNK), BF16),
            pltpu.SemaphoreType.DMA((TP, 2)),
        ],
        compiler_params=params(40),
        cost_estimate=cost(800_000_000, 8_000_000),
        name="shared",
    )(normed, *packed, *shared_left, *shared_right, shared_far_0, shared_far_1)
    return pl.pallas_call(
        combine_kernel,
        out_shape=shape((TOK, D), BF16),
        in_specs=[smem(), smem()] + [vmem()] * 4,
        out_specs=vmem(),
        scratch_shapes=[pltpu.VMEM((TOK * COLS, LANES), F32), pltpu.VMEM((TOK, D), F32)],
        compiler_params=params(40),
        cost_estimate=cost(5_000_000, 4_000_000),
        name="combine",
    )(
        flat_slots, route_weight.T, back.reshape(SLOTS, COLS, LANES),
        shared, residual, moe_gain.reshape(1, -1),
    )


def solution(mesh):
    finer = Mesh(mesh.devices.reshape(8, 4, 2, mesh.shape["tp"]), ("sp_0", "sp_1", "sp_2", "tp"))
    placed = (
        P(SP_TP, None),
        P(SP, "tp"),
        P(SP, "tp"),
        P(SP, "tp"),
        P(SP, "tp"),
        P(SP, "tp"),
        P(SP, "tp"),
        P("tp"),
        P(),
        P(),
        P(),
        P(),
        P(SP_TP, None),
        P(SP_TP, None),
        P(SP, None, "tp"),
        P(SP, None, "tp"),
        P(SP, "tp", None),
        P(None, "tp"),
        P(None, "tp"),
        P("tp", None),
    )

    return jax.shard_map(
        body, mesh=finer, in_specs=placed, out_specs=P(SP_TP, None), check_vma=False
    )
```

```python
import jax
import jax.numpy as jnp
import numpy as np
from jax import lax
from jax.experimental import pallas as pl
from jax.experimental.pallas import tpu as pltpu
from jax.sharding import Mesh
from jax.sharding import PartitionSpec as P


KEY_CHANNELS = 64
DV = 128
BLK = 128
TOPK = 2
CAP = 6
Z, XC, TP = 8, 8, 4
SP = ("sp_0", "sp_1", "sp_2")
PLANE = ("sp_1", "sp_2")
SP_TP = ("sp_0", "sp_1", "sp_2", "tp")
SPAN = 512
TOK = 128
D = 2048
EXPERTS = 64
SLOTS = EXPERTS * CAP
LANES = 128
COLS = D // LANES
CHUNK = 256
PIECES = 4
FAR_PIECES = 4
CHUNKS = D // CHUNK
MSG = 272
HALF_MSG = 144

EPS = 1e-06
GATE_NORM = 16.0
ROPE_BASE = 10000.0
F32 = jnp.float32
BF16 = jnp.bfloat16
NT = (((1,), (1,)), ((), ()))
TN = (((0,), (0,)), ((), ()))


def rope_tables():
    half = KEY_CHANNELS // 2
    frequency = ROPE_BASE ** (-np.arange(half, dtype=np.float64) / half)
    lanes = np.tile(frequency, LANES // half)
    tables = []
    for count, step in ((BLK, 1), (SPAN // BLK, BLK), (Z * XC, SPAN)):
        angles = (np.arange(count) * step)[:, None] * lanes[None, :]
        tables.append(np.stack([np.cos(angles), np.sin(angles)], axis=0).astype(np.float32))
    return tables[0], tables[1].reshape(-1, LANES), tables[2].swapaxes(0, 1)


def dot(a, b, dims=(((1,), (0,)), ((), ()))):
    return lax.dot_general(a, b, dims, preferred_element_type=F32)


def iota(shape, axis):
    return lax.broadcasted_iota(jnp.int32, shape, axis)


def log_sigmoid(x):
    return jnp.minimum(x, 0.0) - jnp.log1p(jnp.exp(-jnp.abs(x)))


def spread(state, low):
    return jnp.concatenate([jnp.where(low, state, 0.0), jnp.where(low, 0.0, state)], axis=0)


def split_rows(rows):
    pieces = []
    for row in rows:
        high = row.astype(BF16)
        pieces += [high.astype(F32), row - high.astype(F32)]
    row_id = iota((16, LANES), 0)
    out = jnp.zeros((16, LANES), F32)
    for i, piece in enumerate(pieces):
        out = jnp.where(row_id == i, piece, out)
    return out


class Block:
    def __init__(self, own_ref, local_ref, block_ref, base_ref):
        self.count = SPAN // BLK
        lane = iota((BLK, LANES), 1)
        self.low = lane < KEY_CHANNELS
        self.front = lane % KEY_CHANNELS < KEY_CHANNELS // 2
        self.row, self.col = iota((BLK, BLK), 0), iota((BLK, BLK), 1)
        self.local, self.blocks = local_ref, block_ref
        self.base = base_ref[own_ref[1] * XC + own_ref[0]]

    def tables(self, n):
        def add(a, b):
            return a[0] * b[0] - a[1] * b[1], a[1] * b[0] + a[0] * b[1]

        span = self.base[0:1, :], self.base[1:2, :]
        m = self.count + n
        start = add(span, (self.blocks[n : n + 1, :], self.blocks[m : m + 1, :]))
        cosine, sine = add(start, (self.local[0], self.local[1]))
        return cosine, jnp.where(self.front, -sine, sine)

    def rotate(self, u, tables):
        swapped = jnp.where(
            self.front,
            pltpu.roll(u, LANES - KEY_CHANNELS // 2, 1),
            pltpu.roll(u, KEY_CHANNELS // 2, 1),
        )
        return u * tables[0] + swapped * tables[1]

    def decays(self, log_ref, forward):
        tri = (self.row >= self.col if forward else self.row <= self.col).astype(BF16)
        parts = []
        for n in range(self.count):
            log = log_sigmoid(log_ref[pl.ds(n * BLK, BLK), :]) * (1.0 / GATE_NORM)
            for _ in range(3):
                part = log.astype(BF16)
                parts.append(part)
                log = log - part.astype(F32)
        sums = dot(tri, jnp.concatenate(parts, axis=1))
        pieces = [sums[:, i * LANES : (i + 1) * LANES] for i in range(3 * self.count)]
        return [sum(pieces[3 * n + 1 : 3 * n + 3], pieces[3 * n]) for n in range(self.count)]


def states_kernel(
    own_ref, k_ref, v_ref, fd_ref, bd_ref, local_ref, block_ref, base_ref,
    msg_ref, key_ref, cumul_ref, states_ref,
):
    block = Block(own_ref, local_ref, block_ref, base_ref)
    count, low = block.count, block.low
    updates, lasts = ([], []), ([], [])
    decays = [block.decays(fd_ref, True), block.decays(bd_ref, False)]
    for n in range(count):
        rows = pl.ds(n * BLK, BLK)
        k = block.rotate(k_ref[rows, :].astype(F32), block.tables(n))
        key_ref[rows, :] = k
        v = v_ref[rows, :]
        for d in range(2):
            cumul = decays[d][n]
            end = BLK - 1 if d == 0 else 0
            total = cumul[end : end + 1, :]
            cumul_ref[d, rows, :] = cumul
            k_out = k * jnp.exp(total - cumul)
            product = dot(v, k_out.astype(BF16), TN)
            updates[d].append(jnp.where(low, product[:DV], product[DV:]))
            lasts[d].append(total)
    finals, sums = [], []
    for d in range(2):
        state, logs = jnp.zeros((DV, LANES), F32), jnp.zeros((1, LANES), F32)
        for n in range(count) if d == 0 else reversed(range(count)):
            states_ref[d, n] = state
            state = state * jnp.exp(lasts[d][n]) + updates[d][n]
            logs = logs + lasts[d][n]
        finals.append(state.astype(BF16))
        sums.append(logs)
    tail = split_rows(sums).astype(BF16)
    for j in range(XC):
        msg_ref[j, pl.ds(0, DV), :] = finals[0]
        msg_ref[j, pl.ds(DV, DV), :] = finals[1]
        msg_ref[j, pl.ds(2 * DV, 16), :] = tail


def attention_kernel(
    own_ref, q_ref, v_ref, key_ref, cumul_ref, states_ref, local_ref, block_ref, base_ref,
    routes_ref,
    part_ref, qdev_ref, slots_ref,
):
    block = Block(own_ref, local_ref, block_ref, base_ref)
    count, low, row, col = block.count, block.low, block.row, block.col
    row2, col2 = iota((BLK, 2 * BLK), 0), iota((BLK, 2 * BLK), 1) % BLK
    wide_low = iota((BLK, 2 * DV), 1) < DV
    zero_row = jnp.zeros((1, LANES), F32)
    lasts = [
        [cumul_ref[0, pl.ds(n * BLK + BLK - 1, 1), :] for n in range(count)],
        [cumul_ref[1, pl.ds(n * BLK, 1), :] for n in range(count)],
    ]
    for n in range(count):
        rows = pl.ds(n * BLK, BLK)
        scale = KEY_CHANNELS ** (-0.5)
        q = block.rotate(q_ref[rows, :].astype(F32) * scale, block.tables(n))
        k = key_ref[rows, :]
        v = v_ref[rows, :].astype(F32)
        v_bd = jnp.concatenate(
            [jnp.where(wide_low, v, 0.0), jnp.where(wide_low, 0.0, v)], axis=0
        ).astype(BF16)
        scores = jnp.zeros((BLK, 2 * BLK), F32)
        q_ins, carried, reaches = [], [], []
        for d in range(2):
            cumul = cumul_ref[d, rows, :]
            at = BLK // 2 - 1 if d == 0 else BLK // 2
            middle = cumul[at : at + 1, :]
            offset = cumul - middle
            q_scaled = q * jnp.exp(offset)
            k_scaled = k * jnp.exp(-offset)
            both = dot(q_scaled.astype(BF16), spread(k_scaled, low).astype(BF16), NT)
            reach = row2 >= col2 if d == 0 else row2 <= col2
            scores = scores + jnp.where(reach, both, 0.0)
            q_ins.append(q_scaled * jnp.exp(middle))
            carried.append(spread(states_ref[d, n], low))
            passed = range(n) if d == 0 else range(n + 1, count)
            reaches.append(sum((lasts[d][m] for m in passed), zero_row))
        q_in = jnp.concatenate(q_ins, axis=1)
        within = dot(scores.astype(BF16), v_bd)
        across = dot(q_in.astype(BF16), jnp.concatenate(carried, axis=1).astype(BF16), NT)
        part_ref[rows, :] = within + across
        qdev_ref[rows, :] = (q_in * jnp.exp(jnp.concatenate(reaches, axis=1))).astype(BF16)

    expert = iota((EXPERTS, TOK), 0)
    picks = [routes_ref[k : k + 1, :] == expert for k in range(TOPK)]
    chosen = jnp.zeros((EXPERTS, TOK), F32)
    for pick in picks:
        chosen = chosen + pick.astype(F32)
    strict = (row < col).astype(BF16)
    before = dot(chosen.astype(BF16), strict)
    place = before + (CAP * expert).astype(F32)
    for k, pick in enumerate(picks):
        found = jnp.sum(jnp.where(pick, place, 0.0), axis=0, keepdims=True)
        slots_ref[k : k + 1, :] = found.astype(jnp.int32)


def compose_gathered(own, gathered_ref, length, shared_place=False):
    results = []
    for forward in (True, False):
        start, tail_at, first = (0, 2 * DV, 0) if forward else (DV, 2 * DV, 2)
        if shared_place:
            start, tail_at, first = 0, DV, 0
        state, logs = jnp.zeros((DV, LANES), F32), jnp.zeros((1, LANES), F32)
        inner, inner_logs = state, logs
        for step in range(length):
            k = step if forward else length - 1 - step
            here = own == k
            inner = jnp.where(here, state, inner)
            inner_logs = jnp.where(here, logs, inner_logs)
            tail = gathered_ref[k, pl.ds(tail_at, 16), :].astype(F32)
            log = tail[first : first + 1, :] + tail[first + 1 : first + 2, :]
            state = state * jnp.exp(log) + gathered_ref[k, pl.ds(start, DV), :].astype(F32)
            logs = logs + log
        results.append((state, logs, inner, inner_logs))
    return results


def plane_kernel(own_ref, gathered_ref, inner_ref, logs_ref, msg_ref):
    forward, backward = compose_gathered(own_ref[0], gathered_ref, XC)
    inner_ref[0] = forward[2]
    inner_ref[1] = backward[2]
    row_id = iota((8, LANES), 0)
    logs_ref[...] = jnp.where(row_id == 0, forward[3], jnp.where(row_id == 1, backward[3], 0.0))
    for j in range(Z):
        later = own_ref[1] < j
        msg_ref[j, pl.ds(0, DV), :] = jnp.where(later, forward[0], backward[0]).astype(BF16)
        logs = jnp.where(later, forward[1], backward[1])
        msg_ref[j, pl.ds(DV, 16), :] = split_rows([logs]).astype(BF16)


def readout_kernel(
    own_ref, gathered_ref, inner_ref, logs_ref, part_ref, qdev_ref, gate_ref, gain_ref, *out_refs
):
    forward, backward = compose_gathered(own_ref[1], gathered_ref, Z, shared_place=True)
    low = iota((DV, LANES), 1) < KEY_CHANNELS
    carry_f = inner_ref[0] + forward[2] * jnp.exp(logs_ref[0:1, :])
    carry_b = inner_ref[1] + backward[2] * jnp.exp(logs_ref[1:2, :])
    carried = jnp.concatenate([spread(carry_f, low), spread(carry_b, low)], axis=1).astype(BF16)
    for n in range(TP):
        rows = pl.ds(pl.multiple_of((own_ref[2] + n) % TP * TOK, TOK), TOK)
        attended = part_ref[rows, :] + dot(qdev_ref[rows, :], carried, NT)
        heads = []
        for h in range(2):
            head = attended[:, h * DV : (h + 1) * DV]
            heads.append(head * lax.rsqrt(jnp.mean(head * head, axis=-1, keepdims=True) + EPS))
        gate = gate_ref[rows, :].astype(F32)
        mixed = jnp.concatenate(heads, axis=1) * gain_ref[...] * (gate * jax.nn.sigmoid(gate))
        out_refs[n][...] = mixed.astype(BF16)


def normalize(x):
    return x * lax.rsqrt(jnp.mean(x * x, axis=-1, keepdims=True) + EPS)


def project_kernel(
    own_ref, slots_ref, mixed_0, mixed_1, mixed_2, mixed_3, weight_ref, stream_ref, mix_ref,
    ffn_ref, residual_ref, normed_ref, sent_ref, acc_ref, rows_ref,
):
    step = pl.program_id(0)

    @pl.when(step == 0)
    def _():
        acc_ref[...] = dot(mixed_0[...], weight_ref[...])
        sent_ref[...] = jnp.zeros_like(sent_ref)

    for n, mixed_ref in enumerate((mixed_1, mixed_2, mixed_3)):

        @pl.when(step == n + 1)
        def _(mixed_ref=mixed_ref):
            acc_ref[...] += dot(mixed_ref[...], weight_ref[...])

    @pl.when(step == TP - 1)
    def _():
        projected = normalize(acc_ref[...]) * mix_ref[...]
        residual = (stream_ref[...].astype(F32) + projected).astype(BF16)
        residual_ref[...] = residual
        normed = (normalize(residual.astype(F32)) * ffn_ref[...]).astype(BF16)
        normed_ref[...] = normed
        wide = normed.astype(F32)
        for j in range(COLS):
            rows_ref[pl.ds(j, TOK, stride=COLS), :] = wide[:, j * LANES : (j + 1) * LANES]

        def place(t, carry):
            line = rows_ref[pl.ds(pl.multiple_of(t * COLS, COLS), COLS), :].astype(BF16)
            for k in range(TOPK):
                sent_ref[slots_ref[k, t]] = line
            return carry

        lax.fori_loop(0, TOK, place, 0, unroll=8)


def pack_shared_kernel(gate_ref, up_ref, down_ref, after_ref, *out_refs):
    half = CHUNKS // 2
    for i in range(CHUNKS):
        rows = pl.ds(i * CHUNK, CHUNK)
        out_ref, at = out_refs[i // half], i % half
        out_ref[at, pl.ds(0, CHUNK), pl.ds(0, LANES)] = gate_ref[rows, :]
        out_ref[at, pl.ds(0, CHUNK), pl.ds(LANES, LANES)] = up_ref[rows, :]
        out_ref[at, pl.ds(CHUNK, LANES), :] = down_ref[:, rows]


def pack_shared(gate, up, down, after):
    return pl.pallas_call(
        pack_shared_kernel,
        out_shape=(shape((CHUNKS // 2, CHUNK + LANES, CHUNK), BF16),) * 2,
        in_specs=[vmem()] * 3 + [anywhere()],
        out_specs=(vmem(),) * 2,
        compiler_params=params(),
        cost_estimate=cost(1_000_000, 3_200_000),
        name="pack_shared",
    )(gate, up, down, after)


def silu(x):
    return x * jax.nn.sigmoid(x)


def expert_copies(gates, ups, downs, gate_ref, up_ref, down_ref, sems):
    copies = []
    for n in range(len(gates)):
        copies.append([
            pltpu.make_async_copy(gates[n], gate_ref.at[n], sems.at[0, n]),
            pltpu.make_async_copy(ups[n], up_ref.at[n], sems.at[1, n]),
        ])
        if len(downs) == len(gates):
            copies[n].append(pltpu.make_async_copy(downs[n], down_ref.at[n], sems.at[2, n]))
        else:
            half = down_ref.shape[1] // 2
            copies[n] += [
                pltpu.make_async_copy(
                    downs[h], down_ref.at[n, pl.ds(h * half, half)], sems.at[2 + h, n]
                )
                for h in range(2)
            ]
    for group in copies:
        for copy in group:
            copy.start()
    return copies


def expert_near_kernel(*refs):
    sent_ref, gates, ups, downs = refs[0], refs[1:4], refs[4:7], refs[7:10]
    rows_ref, acc_ref, sent, lines_ref, gate_ref, up_ref, down_ref, sent_sems, sems = refs[10:]
    part = SLOTS // PIECES
    arrivals = [
        pltpu.make_async_copy(
            sent_ref.at[pl.ds(p * part * COLS, part * COLS)],
            sent.at[pl.ds(p * part * COLS, part * COLS)],
            sent_sems.at[p],
        )
        for p in range(PIECES)
    ]
    for copy in arrivals:
        copy.start()
    copies = expert_copies(gates, ups, downs, gate_ref, up_ref, down_ref, sems)
    for p, copy in enumerate(arrivals):
        copy.wait()
        span = pl.ds(p * part * COLS, part * COLS)
        lines_ref[span, :] = sent[span, :].astype(F32)
        for j in range(COLS):
            rows_ref[pl.ds(p * part, part), j * LANES : (j + 1) * LANES] = lines_ref[
                pl.ds(p * part * COLS + j, part, stride=COLS), :
            ].astype(BF16)
    for n, group in enumerate(copies):
        group[0].wait()
        group[1].wait()
        rows = rows_ref[...]
        hidden = (silu(dot(rows, gate_ref[n])) * dot(rows, up_ref[n])).astype(BF16)
        group[2].wait()
        for j in range(CHUNKS):
            columns = pl.ds(j * CHUNK, CHUNK)
            product = dot(hidden, down_ref[n, :, columns])
            if n == 0:
                acc_ref[:, columns] = product
            else:
                acc_ref[:, columns] += product


def expert_far_kernel(*refs):
    rows_ref, acc_ref, gates, ups, downs, out_ref = refs[0], refs[1], refs[2:3], refs[3:4], refs[4:6], refs[6]
    sent, lines_ref, gate_ref, up_ref, down_ref, sems, out_sems = refs[7:]
    part = SLOTS // FAR_PIECES
    group = expert_copies(gates, ups, downs, gate_ref, up_ref, down_ref, sems)[0]
    for copy in group:
        copy.wait()
    rows = rows_ref[...]
    hidden = (silu(dot(rows, gate_ref[0])) * dot(rows, up_ref[0])).astype(BF16)
    for j in range(CHUNKS):
        columns = pl.ds(j * CHUNK, CHUNK)
        total = acc_ref[:, columns] + dot(hidden, down_ref[0, :, columns])
        for i in range(CHUNK // LANES):
            lines_ref[pl.ds(j * (CHUNK // LANES) + i, SLOTS, stride=COLS), :] = total[
                :, i * LANES : (i + 1) * LANES
            ]
    outs = []
    for p in range(FAR_PIECES):
        span = pl.ds(p * part * COLS, part * COLS)
        sent[span, :] = lines_ref[span, :].astype(BF16)
        copy = pltpu.make_async_copy(sent.at[span], out_ref.at[span], out_sems.at[p])
        copy.start()
        outs.append(copy)
    for copy in outs:
        copy.wait()


def shared_kernel(*refs):
    rows_ref, shards, out_ref, weight_ref, sems = refs[0], refs[1:9], refs[9], refs[10], refs[11]
    half = CHUNKS // 2
    copies = [
        pltpu.make_async_copy(
            shards[2 * n + h], weight_ref.at[n, pl.ds(h * half, half)], sems.at[n, h]
        )
        for n in range(TP)
        for h in range(2)
    ]
    for copy in copies:
        copy.start()
    for n in range(TP):
        copies[2 * n].wait()
        copies[2 * n + 1].wait()
        joint = jnp.zeros((TOK, 2 * LANES), F32)
        for i in range(CHUNKS):
            columns = pl.ds(i * CHUNK, CHUNK)
            joint = joint + dot(rows_ref[:, columns], weight_ref[n, i, 0:CHUNK, :])
        hidden = (silu(joint[:, :LANES]) * joint[:, LANES:]).astype(BF16)
        for i in range(CHUNKS):
            columns = pl.ds(i * CHUNK, CHUNK)
            product = dot(hidden, weight_ref[n, i, CHUNK:, :])
            if n == 0:
                out_ref[:, columns] = product
            else:
                out_ref[:, columns] += product


def combine_kernel(
    slots_ref, weights_ref, back_ref, shared_ref, residual_ref, gain_ref, out_ref, lines_ref, mix_ref
):
    def gather(t, carry):
        line = jnp.zeros((COLS, LANES), F32)
        for k in range(TOPK):
            line = line + back_ref[slots_ref[k, t]].astype(F32) * weights_ref[k, t]
        lines_ref[pl.ds(pl.multiple_of(t * COLS, COLS), COLS), :] = line
        return carry

    lax.fori_loop(0, TOK, gather, 0, unroll=8)
    for j in range(COLS):
        columns = slice(j * LANES, (j + 1) * LANES)
        mix_ref[:, columns] = shared_ref[:, columns] + lines_ref[pl.ds(j, TOK, stride=COLS), :]
    out_ref[...] = (
        residual_ref[...].astype(F32) + normalize(mix_ref[...]) * gain_ref[...]
    ).astype(BF16)


def vmem():
    return pl.BlockSpec(memory_space=pltpu.VMEM)


def anywhere():
    return pl.BlockSpec(memory_space=pltpu.HBM)


def shift(array, hops):
    return lax.ppermute(array, "tp", [(i, (i + hops) % TP) for i in range(TP)])


def smem():
    return pl.BlockSpec(memory_space=pltpu.SMEM)


def params(mib=60, **extra):
    return pltpu.CompilerParams(vmem_limit_bytes=mib * 1024 * 1024, **extra)


def shape(dims, kind):
    return jax.ShapeDtypeStruct(dims, kind)


def cost(flops, moved):
    return pl.CostEstimate(flops=flops, bytes_accessed=moved, transcendentals=0)


def whole(dims):
    return pl.BlockSpec(dims, lambda i, *_: (0,) * len(dims))


def body(
    stream,
    queries,
    key_rows,
    values,
    out_gate,
    fwd_decay,
    bwd_decay,
    head_gain,
    out_proj,
    mix_gain,
    ffn_gain,
    moe_gain,
    routes,
    route_weight,
    expert_gate,
    expert_up,
    expert_down,
    shared_gate,
    shared_up,
    shared_down,
):
    own = jnp.stack([lax.axis_index(axes) for axes in (PLANE, "sp_0", "tp", "sp_2")])
    own = own.astype(jnp.int32)
    gate, up, down = expert_gate[0], expert_up[0], expert_down[0]
    gate_left = shift(gate, 1)
    gate_right = shift(gate, -1)
    up_left = shift(up, 1)
    up_right = shift(up, -1)

    tables = [jnp.asarray(table) for table in rope_tables()]
    msg, keys, cumuls, states = pl.pallas_call(
        states_kernel,
        out_shape=(
            shape((XC, MSG, LANES), BF16),
            shape((SPAN, LANES), F32),
            shape((2, SPAN, LANES), F32),
            shape((2, SPAN // BLK, DV, LANES), F32),
        ),
        in_specs=[smem()] + [vmem()] * 7,
        out_specs=(vmem(),) * 4,
        compiler_params=params(),
        cost_estimate=cost(200_000_000, 4_000_000),
        name="states",
    )(own, key_rows, values, fwd_decay, bwd_decay, *tables)
    in_plane = lax.all_to_all(msg, PLANE, split_axis=0, concat_axis=0, tiled=True)
    part, qdev, flat_slots = pl.pallas_call(
        attention_kernel,
        out_shape=(
            shape((SPAN, 2 * DV), F32),
            shape((SPAN, 2 * LANES), BF16),
            shape((TOPK, TOK), jnp.int32),
        ),
        in_specs=[smem()] + [vmem()] * 9,
        out_specs=(vmem(),) * 3,
        compiler_params=params(),
        cost_estimate=cost(400_000_000, 4_000_000),
        name="attention",
    )(own, queries, values, keys, cumuls, states, *tables, routes.T)
    inner, logs, msg = pl.pallas_call(
        plane_kernel,
        out_shape=(
            shape((2, DV, LANES), F32),
            shape((8, LANES), F32),
            shape((Z, HALF_MSG, LANES), BF16),
        ),
        in_specs=[smem(), vmem()],
        out_specs=(vmem(),) * 3,
        compiler_params=params(40),
        cost_estimate=cost(10_000_000, 1_000_000),
        name="plane",
    )(own, in_plane)
    planes = lax.all_to_all(msg, "sp_0", split_axis=0, concat_axis=0, tiled=True)
    mixed = pl.pallas_call(
        readout_kernel,
        out_shape=(shape((TOK, 2 * DV), BF16),) * TP,
        in_specs=[smem()] + [vmem()] * 7,
        out_specs=(vmem(),) * TP,
        compiler_params=params(60),
        cost_estimate=cost(100_000_000, 3_000_000),
        name="readout",
    )(
        own, planes, inner, logs, part, qdev, out_gate, head_gain.reshape(1, -1),
    )
    mixed = [shift(piece, n) if n else piece for n, piece in enumerate(mixed)]

    down_left = shift(down, 1)
    down_right = shift(down, -1)
    gate_far = shift(gate_left, 1)
    up_far = shift(up_right, -1)
    down_far_1 = shift(down_left[: down.shape[0] // 2], 1)
    down_far_2 = shift(down_right[down.shape[0] // 2 :], -1)

    residual, normed, sent = pl.pallas_call(
        project_kernel,
        out_shape=(
            shape((TOK, D), BF16),
            shape((TOK, D), BF16),
            shape((SLOTS, COLS, LANES), BF16),
        ),
        grid_spec=pltpu.PrefetchScalarGridSpec(
            num_scalar_prefetch=2,
            grid=(TP,),
            in_specs=[whole((TOK, 2 * DV))] * TP
            + [
                pl.BlockSpec((2 * DV, D), lambda i, own, _: ((own[2] + TP - i) % TP, 0)),
                whole((TOK, D)),
                whole((1, D)),
                whole((1, D)),
            ],
            out_specs=(whole((TOK, D)), whole((TOK, D)), whole((SLOTS, COLS, LANES))),
            scratch_shapes=[pltpu.VMEM((TOK, D), F32), pltpu.VMEM((TOK * COLS, LANES), F32)],
        ),
        compiler_params=params(59, dimension_semantics=("arbitrary",)),
        cost_estimate=cost(600_000_000, 8_000_000),
        name="project",
    )(own, flat_slots, *mixed, out_proj, stream, mix_gain.reshape(1, -1), ffn_gain.reshape(1, -1))

    arrived = lax.all_to_all(
        sent.reshape(EXPERTS, CAP * COLS, LANES), SP, split_axis=0, concat_axis=0, tiled=True
    )
    width = gate.shape[1]
    near = TP - 1
    rows, partial = pl.pallas_call(
        expert_near_kernel,
        out_shape=(shape((SLOTS, D), BF16), shape((SLOTS, D), F32)),
        in_specs=[anywhere()] * (1 + 3 * near),
        out_specs=(vmem(), vmem()),
        scratch_shapes=[
            pltpu.VMEM((SLOTS * COLS, LANES), BF16),
            pltpu.VMEM((SLOTS * COLS, LANES), F32),
            pltpu.VMEM((near, D, width), BF16),
            pltpu.VMEM((near, D, width), BF16),
            pltpu.VMEM((near, width, D), BF16),
            pltpu.SemaphoreType.DMA((PIECES,)),
            pltpu.SemaphoreType.DMA((3, near)),
        ],
        compiler_params=params(26),
        cost_estimate=cost(3_600_000_000, 16_000_000),
        name="experts_near",
    )(
        arrived.reshape(SLOTS * COLS, LANES),
        gate, gate_left, gate_right, up, up_left, up_right, down, down_left, down_right,
    )
    done = pl.pallas_call(
        expert_far_kernel,
        out_shape=shape((SLOTS * COLS, LANES), BF16),
        in_specs=[vmem(), vmem()] + [anywhere()] * 4,
        out_specs=anywhere(),
        scratch_shapes=[
            pltpu.VMEM((SLOTS * COLS, LANES), BF16),
            pltpu.VMEM((SLOTS * COLS, LANES), F32),
            pltpu.VMEM((1, D, width), BF16),
            pltpu.VMEM((1, D, width), BF16),
            pltpu.VMEM((1, width, D), BF16),
            pltpu.SemaphoreType.DMA((4, 1)),
            pltpu.SemaphoreType.DMA((FAR_PIECES,)),
        ],
        compiler_params=params(20),
        cost_estimate=cost(1_200_000_000, 8_000_000),
        name="experts_far",
    )(rows, partial, gate_far, up_far, down_far_1, down_far_2)
    back = lax.all_to_all(
        done.reshape(EXPERTS, CAP * COLS, LANES), SP, split_axis=0, concat_axis=0, tiled=True
    )
    packed = pack_shared(shared_gate, shared_up, shared_down, residual)
    shared_left, shared_right = [None, None], [None, None]
    for h in range(2):
        shared_left[h] = shift(packed[h], 1)
        shared_right[h] = shift(packed[h], -1)
    shared_far_0 = shift(shared_left[0], 1)
    shared_far_1 = shift(shared_right[1], -1)
    shared = pl.pallas_call(
        shared_kernel,
        out_shape=shape((TOK, D), F32),
        in_specs=[vmem()] + [anywhere()] * 8,
        out_specs=vmem(),
        scratch_shapes=[
            pltpu.VMEM((TP, CHUNKS, CHUNK + LANES, CHUNK), BF16),
            pltpu.SemaphoreType.DMA((TP, 2)),
        ],
        compiler_params=params(40),
        cost_estimate=cost(800_000_000, 8_000_000),
        name="shared",
    )(normed, *packed, *shared_left, *shared_right, shared_far_0, shared_far_1)
    return pl.pallas_call(
        combine_kernel,
        out_shape=shape((TOK, D), BF16),
        in_specs=[smem(), smem()] + [vmem()] * 4,
        out_specs=vmem(),
        scratch_shapes=[pltpu.VMEM((TOK * COLS, LANES), F32), pltpu.VMEM((TOK, D), F32)],
        compiler_params=params(40),
        cost_estimate=cost(5_000_000, 4_000_000),
        name="combine",
    )(
        flat_slots, route_weight.T, back.reshape(SLOTS, COLS, LANES),
        shared, residual, moe_gain.reshape(1, -1),
    )


def solution(mesh):
    finer = Mesh(mesh.devices.reshape(8, 4, 2, mesh.shape["tp"]), ("sp_0", "sp_1", "sp_2", "tp"))
    placed = (
        P(SP_TP, None),
        P(SP, "tp"),
        P(SP, "tp"),
        P(SP, "tp"),
        P(SP, "tp"),
        P(SP, "tp"),
        P(SP, "tp"),
        P("tp"),
        P(),
        P(),
        P(),
        P(),
        P(SP_TP, None),
        P(SP_TP, None),
        P(SP, None, "tp"),
        P(SP, None, "tp"),
        P(SP, "tp", None),
        P(None, "tp"),
        P(None, "tp"),
        P("tp", None),
    )

    return jax.shard_map(
        body, mesh=finer, in_specs=placed, out_specs=P(SP_TP, None), check_vma=False
    )
```
